128 devices in a mesh: sp: 32 (over z, y, core), tp: 4 (over x).
Axes of the slice: x: 4, y: 4, z: 4, core: 2. Of those that a mesh axis runs over, the one named last changes fastest.
Arguments:
- residual_input_stream: bfloat16 [32768, 2048], P(('sp', 'tp')), may hold values from -6 to 6
- receptance: bfloat16 [32768, 1024], P('sp', 'tp'), may hold values from -6 to 6
- key_matrix_all: bfloat16 [32768, 1024], P('sp', 'tp'), may hold values from -6 to 6
- value_matrix_all: bfloat16 [32768, 1024], P('sp', 'tp'), may hold values from -6 to 6
- decay_preactivation: bfloat16 [32768, 1024], P('sp', 'tp'), may hold values from -15 to 1
- learning_rate_preactivation: bfloat16 [32768, 1024], P('sp', 'tp'), may hold values from -11 to 5
- output_gate_all_heads: bfloat16 [32768, 1024], P('sp', 'tp'), may hold values from -6 to 6
- extra_log_decay: float32 [32768, 1024], P('sp', 'tp'), may hold values from -0.7 to 0
- head_norm_gain: float32 [1024], P('tp'), may hold values from 0.1 to 1.9
- output_projection_weight: bfloat16 [1024, 2048], P('tp'), may hold values from -0.1875 to 0.1875
- feedforward_norm_gain: float32 [2048], replicated, may hold values from 0.1 to 1.9
- gate_projection_weight: bfloat16 [2048, 5632], P('sp', 'tp'), may hold values from -0.125 to 0.125
- up_projection_weight: bfloat16 [2048, 5632], P('sp', 'tp'), may hold values from -0.125 to 0.125
- down_projection_weight: bfloat16 [2048, 5632], P('sp', 'tp'), may hold values from -0.078125 to 0.078125
- convolution_kernel: bfloat16 [3, 2, 5632], P(None, None, 'tp'), may hold values from -3.5 to 3.5
Outputs:
- layer_out: bfloat16 [32768, 2048], P(('sp', 'tp'))
The draws below stay inside these ranges and needn't reach their ends.
All inputs are finite; a program needn't handle non-finite values.
Results may differ from the reference program's by a relative error of at most 0.022.
Values may be sent and summed in bfloat16 or wider, within the bound.
No kernel may reach another device: no remote copies, remote signals or barrier semaphores. Data moves between devices by JAX's collectives and lax.ppermute only.
A program may use at most 128 MiB of HBM per device.

```python
import math
import jax
import jax.numpy as jnp
from jax import lax

D = 2048
HEAD_TOTAL = 16
HEAD_WIDTH = 64
FF = 5632
TOK_DEV = 1024
TOKEN_TOTAL = 32768
N_TP = 4


def slow_heads(key):
    share = 0.5
    return jax.random.uniform(jax.random.fold_in(key, 7), (HEAD_TOTAL,)) < share


def head_noise(key, scale):
    return scale * jax.random.truncated_normal(key, -4.0, 4.0, (TOKEN_TOTAL, HEAD_TOTAL * HEAD_WIDTH), jnp.float32)


def draw_decay_preactivation(key, part):
    slow = slow_heads(key)
    base = jnp.repeat(jnp.where(slow, -10.5, -3.2), HEAD_WIDTH)
    noise = head_noise(jax.random.fold_in(key, 1), 0.8)
    offsets = jax.random.uniform(jax.random.fold_in(key, 2), (TOKEN_TOTAL // TOK_DEV, 1), jnp.float32, -0.8, 0.8)
    return (base[None, :] + noise + jnp.repeat(offsets, TOK_DEV, axis=0)).astype(jnp.bfloat16)


def draw_learning_rate_preactivation(key, part):
    slow = slow_heads(key)
    base = jnp.repeat(jnp.where(slow, -6.5, 0.5), HEAD_WIDTH)
    noise = head_noise(jax.random.fold_in(key, 3), 1.0)
    return (base[None, :] + noise).astype(jnp.bfloat16)


def draw_extra_log_decay(key, part):
    hits = jax.random.uniform(jax.random.fold_in(key, 4), (TOKEN_TOTAL, HEAD_TOTAL)) < 4.0 / TOKEN_TOTAL
    values = jax.random.uniform(jax.random.fold_in(key, 5), (TOKEN_TOTAL, HEAD_TOTAL * HEAD_WIDTH), jnp.float32, math.log(0.5), math.log(0.8))
    return jnp.where(jnp.repeat(hits, HEAD_WIDTH, axis=1), values, 0.0)


def level_of(own_key, shape, shards, least, high):
    def one(axis_at, parts):
        draws = jax.random.uniform(jax.random.fold_in(jax.random.fold_in(own_key, 6), axis_at), (parts,), jnp.float32, least / len(shards), high / len(shards))
        return jnp.repeat(jnp.exp(draws), shape[axis_at] // parts).reshape((-1,) + (1,) * (len(shape) - axis_at - 1))

    level = one(*shards[0])
    for cut in shards[1:]:
        level = level * one(*cut)
    return level


def scatter_about(key, shape, scale, bound, shards=(), dtype=jnp.bfloat16):
    array = scale * jax.random.normal(key, shape, jnp.float32)
    if shards:
        array = array * level_of(key, shape, shards, -0.22, 0.18)
    return jnp.clip(array, -bound, bound).astype(dtype)


def setup_inputs(seed: int = 0) -> dict:
    streams_of = jax.random.split(jax.random.key(seed), 16)
    return {
        "residual_input_stream": scatter_about(streams_of[0], (TOKEN_TOTAL, D), 1.0, 6.0, ((0, 128),)),
        "receptance": scatter_about(streams_of[1], (TOKEN_TOTAL, HEAD_TOTAL * HEAD_WIDTH), 1.0, 6.0, ((0, 32), (1, 4))),
        "key_matrix_all": scatter_about(streams_of[2], (TOKEN_TOTAL, HEAD_TOTAL * HEAD_WIDTH), 1.0, 6.0, ((0, 32), (1, 4))),
        "value_matrix_all": scatter_about(streams_of[3], (TOKEN_TOTAL, HEAD_TOTAL * HEAD_WIDTH), 1.0, 6.0, ((0, 32), (1, 4))),
        "decay_preactivation": draw_decay_preactivation(jax.random.fold_in(streams_of[15], 71), 0),
        "learning_rate_preactivation": draw_learning_rate_preactivation(jax.random.fold_in(streams_of[15], 71), 0),
        "output_gate_all_heads": scatter_about(streams_of[6], (TOKEN_TOTAL, HEAD_TOTAL * HEAD_WIDTH), 1.0, 6.0, ((0, 32), (1, 4))),
        "extra_log_decay": draw_extra_log_decay(jax.random.fold_in(streams_of[15], 71), 0),
        "head_norm_gain": jnp.clip(1.0 + 0.18 * jax.random.normal(streams_of[8], (HEAD_TOTAL * HEAD_WIDTH,), jnp.float32), 0.1, 1.9),
        "output_projection_weight": scatter_about(streams_of[9], (HEAD_TOTAL * HEAD_WIDTH, D), (HEAD_TOTAL * HEAD_WIDTH) ** -0.5, 0.1875, ((0, 4),)),
        "feedforward_norm_gain": jnp.clip(1.0 + 0.18 * jax.random.normal(streams_of[10], (D,), jnp.float32), 0.1, 1.9),
        "gate_projection_weight": scatter_about(streams_of[11], (D, FF), D ** -0.5, 0.125, ((0, 32), (1, 4))),
        "up_projection_weight": scatter_about(streams_of[12], (D, FF), D ** -0.5, 0.125, ((0, 32), (1, 4))),
        "down_projection_weight": scatter_about(streams_of[13], (D, FF), FF ** -0.5, 0.078125, ((0, 32), (1, 4))),
        "convolution_kernel": scatter_about(streams_of[14], (3, 2, FF), 0.577, 3.5, ((2, 4),)),
    }


highest = lax.Precision.HIGHEST

def per_head_layout(values_in):
    return values_in.astype(jnp.float32).reshape(values_in.shape[0], HEAD_TOTAL, HEAD_WIDTH)

def reference(residual_input_stream, receptance, key_matrix_all, value_matrix_all, decay_preactivation, learning_rate_preactivation, output_gate_all_heads, extra_log_decay, head_norm_gain, output_projection_weight, feedforward_norm_gain, gate_projection_weight, up_projection_weight, down_projection_weight, convolution_kernel):
    queries = per_head_layout(receptance)
    keys = per_head_layout(key_matrix_all)
    values = per_head_layout(value_matrix_all)
    decay_logarithm = -jnp.exp(-jax.nn.softplus(-per_head_layout(decay_preactivation)) - 0.5) + extra_log_decay.reshape(TOKEN_TOTAL, HEAD_TOTAL, HEAD_WIDTH)
    factors = jnp.exp(decay_logarithm)
    rates = jax.nn.sigmoid(per_head_layout(learning_rate_preactivation))
    normed_keys = keys * lax.rsqrt(lax.optimization_barrier(jnp.sum(keys * keys, axis=-1, keepdims=True)) + 1e-06)
    removal = normed_keys * rates

    def advance(carried, inputs_now):
        query_now, key_now, value_now, factor_now, normed_now, removal_now = inputs_now
        along = jnp.einsum('hvk,hk->hv', carried, normed_now, precision=highest)
        carried = carried * factor_now[:, None, :] - along[:, :, None] * removal_now[:, None, :] + value_now[:, :, None] * key_now[:, None, :]
        return (carried, jnp.einsum('hvk,hk->hv', carried, query_now, precision=highest))
    start_state = jnp.zeros((HEAD_TOTAL, HEAD_WIDTH, HEAD_WIDTH), jnp.float32)
    final_state, readout = lax.scan(advance, start_state, (queries, keys, values, factors, normed_keys, removal))
    centered = readout - lax.optimization_barrier(jnp.mean(readout, axis=-1, keepdims=True))
    variance = lax.optimization_barrier(jnp.mean(centered * centered, axis=-1, keepdims=True))
    normalized = (centered * lax.rsqrt(variance + 0.00064)).reshape(TOKEN_TOTAL, HEAD_TOTAL * HEAD_WIDTH)
    mixed_out = (normalized * head_norm_gain * output_gate_all_heads.astype(jnp.float32)).astype(jnp.bfloat16)
    group_width = HEAD_TOTAL * HEAD_WIDTH // N_TP
    attention = jnp.zeros((TOKEN_TOTAL, D), jnp.float32)
    for group in range(N_TP):
        part = jnp.dot(mixed_out[:, group * group_width:(group + 1) * group_width], output_projection_weight[group * group_width:(group + 1) * group_width], preferred_element_type=jnp.float32)
        attention = attention + lax.optimization_barrier(part.astype(jnp.bfloat16)).astype(jnp.float32)
    stream = lax.optimization_barrier((residual_input_stream.astype(jnp.float32) + attention).astype(jnp.bfloat16))
    stream_wide = stream.astype(jnp.float32)
    normed = (stream_wide * lax.rsqrt(lax.optimization_barrier(jnp.mean(stream_wide * stream_wide, axis=-1, keepdims=True)) + 1e-06) * feedforward_norm_gain).astype(jnp.bfloat16)
    taps = convolution_kernel.astype(jnp.float32)
    unit_width = FF // N_TP
    block_count = TOKEN_TOTAL // TOK_DEV

    def ffn_block(carried, inputs_now):
        normed_block, stream_block = inputs_now
        gate_pre = jnp.dot(normed_block, gate_projection_weight, preferred_element_type=jnp.float32).astype(jnp.bfloat16)
        up_pre = jnp.dot(normed_block, up_projection_weight, preferred_element_type=jnp.float32).astype(jnp.bfloat16)
        gate_ext = jnp.concatenate([carried[0], gate_pre], axis=0).astype(jnp.float32)
        up_ext = jnp.concatenate([carried[1], up_pre], axis=0).astype(jnp.float32)
        gate_mix = taps[0, 0] * gate_ext[:-2] + taps[1, 0] * gate_ext[1:-1] + taps[2, 0] * gate_ext[2:]
        up_mix = taps[0, 1] * up_ext[:-2] + taps[1, 1] * up_ext[1:-1] + taps[2, 1] * up_ext[2:]
        hidden = (jax.nn.silu(gate_mix) * up_mix).astype(jnp.bfloat16)
        ffn = jnp.zeros((TOK_DEV, D), jnp.float32)
        for group in range(N_TP):
            part = jnp.dot(hidden[:, group * unit_width:(group + 1) * unit_width], down_projection_weight[:, group * unit_width:(group + 1) * unit_width].T, preferred_element_type=jnp.float32)
            ffn = ffn + lax.optimization_barrier(part.astype(jnp.bfloat16)).astype(jnp.float32)
        layer_block = (stream_block.astype(jnp.float32) + ffn).astype(jnp.bfloat16)
        return ((gate_pre[-2:], up_pre[-2:]), layer_block)
    start_rows = (jnp.zeros((2, FF), jnp.bfloat16), jnp.zeros((2, FF), jnp.bfloat16))
    last_rows, layer_blocks = lax.scan(ffn_block, start_rows, (normed.reshape(block_count, TOK_DEV, D), stream.reshape(block_count, TOK_DEV, D)))
    return layer_blocks.reshape(TOKEN_TOTAL, D)
```

```python
import jax
import jax.numpy as jnp
from jax import lax
from jax.experimental import pallas as pl
from jax.experimental.pallas import tpu as pltpu
from jax.sharding import Mesh
from jax.sharding import PartitionSpec as P

SP = ("sp_0", "sp_1", "sp_2")
SP_TP = ("sp_0", "sp_1", "sp_2", "tp")

BF = jnp.bfloat16
F32 = jnp.float32
CHUNK = 64
GROUP = 4
ROWS = CHUNK * GROUP


def mm(a, b):
    return lax.dot_general(a, b, (((1,), (0,)), ((), ())), preferred_element_type=F32)


def mm_nt(a, b):
    return lax.dot_general(a, b, (((1,), (1,)), ((), ())), preferred_element_type=F32)


def split2(x):
    hi = x.astype(BF)
    return hi, (x - hi.astype(F32)).astype(BF)


def mm3(a, b):
    ah, al = split2(a)
    bh, bl = split2(b)
    return mm(ah, bh) + (mm(ah, bl) + mm(al, bh))


def iotas(n, m):
    return lax.broadcasted_iota(jnp.int32, (n, m), 0), lax.broadcasted_iota(jnp.int32, (n, m), 1)


def head_ones(n):
    i, j = iotas(n, n)
    return jnp.where((i // 64) == (j // 64), 1.0, 0.0).astype(BF)


def head_sum(x, ones):
    hi, lo = split2(x)
    return mm(hi, ones) + mm(lo, ones)


def block_diagonal(n):
    i, j = iotas(n, n)
    return (i // 64) == (j // 64)


def pack_map(m, b):
    i, j = iotas(128, 128)
    e = m - jnp.where(i == j, 1.0, 0.0)
    return jnp.where(j < 64, e + pltpu.roll(e, 64, 1), b + pltpu.roll(b, 64, 1)).astype(BF)


def unpack_map(p):
    i, j = iotas(128, 128)
    p = p.astype(F32)
    s = pltpu.roll(p, 64, 1)
    bd = (i // 64) == (j // 64)
    m = jnp.where(bd, jnp.where(j < 64, p, s), 0.0) + jnp.where(i == j, 1.0, 0.0)
    b = jnp.where(bd, jnp.where(j < 64, s, p), 0.0)
    return m, b


def compose(first, second):
    both = mm3(second[0], jnp.concatenate([first[0], first[1]], axis=1))
    return both[:, :128], both[:, 128:] + second[1]


def chunk_kernel(r_ref, k_ref, v_ref, d_ref, a_ref, x_ref, q_ref, o_ref, mc_ref, bc_ref, mg_ref, bg_ref, pk_ref):
    step = pl.program_id(0)
    ones = head_ones(256)
    k = k_ref[...].astype(F32)
    n = k * lax.rsqrt(head_sum(k * k, ones) + 1e-6)
    rate = 1.0 / (1.0 + jnp.exp(-a_ref[...].astype(F32)))
    b = n * rate
    ld = (-0.6065306597126334) / (1.0 + jnp.exp(-d_ref[...].astype(F32))) + x_ref[...]
    i, j = iotas(ROWS, ROWS)
    tri = jnp.where(((i // CHUNK) == (j // CHUNK)) & (i >= j), 1.0, 0.0).astype(BF)
    ldh, ldl = split2(ld)
    g = mm(tri, ldh) + mm(tri, ldl)
    mids = [g[c * CHUNK + CHUNK // 2 : c * CHUNK + CHUNK // 2 + 1] for c in range(GROUP)]
    ends = [g[c * CHUNK + CHUNK - 1 : c * CHUNK + CHUNK] for c in range(GROUP)]
    rel = jnp.concatenate([g[c * CHUNK : (c + 1) * CHUNK] - mids[c] for c in range(GROUP)], axis=0)
    up = jnp.exp(rel)
    prev = jnp.exp(rel - ld)
    down = jnp.exp(-rel)
    rq = r_ref[...].astype(F32) * up
    nq = n * prev
    kk = k * down
    bb = b * down
    v = v_ref[...]

    i, j = iotas(128, 128)
    bd = (i // 64) == (j // 64)
    ti, tj = i % 64, j % 64
    strict = bd & (ti > tj)
    within = bd & (ti >= tj)
    eye = jnp.where(i == j, 1.0, 0.0)
    mask_a = jnp.concatenate([jnp.concatenate([strict, strict], axis=1), jnp.concatenate([within, within], axis=1)], axis=0)
    low = lax.broadcasted_iota(jnp.int32, (64, 128), 1) < 64
    zero = jnp.zeros((64, 128), BF)

    def spread(x):
        return jnp.concatenate([jnp.where(low, x, zero), jnp.where(low, zero, x)], axis=0)

    def fold(x):
        return jnp.where(low, x[:64], x[64:])

    units = [(c, p) for c in range(GROUP) for p in range(2)]

    def cut(x, u):
        c, p = u
        return x[c * CHUNK : (c + 1) * CHUNK, p * 128 : (p + 1) * 128]

    st = {}
    for u in units:
        nqb = spread(cut(nq, u).astype(BF))
        rqb = spread(cut(rq, u).astype(BF))
        kb = cut(kk, u).astype(BF)
        bbb = cut(bb, u).astype(BF)
        vb = cut(v, u)
        vs = spread(vb)
        att = mm_nt(jnp.concatenate([nqb, rqb], axis=0), jnp.concatenate([kb, kb, bbb, bbb], axis=0))
        att = jnp.where(mask_a, att, 0.0)
        kv = mm(att[:, :128].astype(BF), vs)
        st[u] = dict(nqb=nqb, rqb=rqb, vb=vb, L=att[:128, 128:], arb=att[128:, 128:].astype(BF), av=kv[:128], ov=kv[128:])
    lev = jnp.where(bd & ((ti // 2) == (tj // 2)), 1.0, 0.0)
    for u in units:
        st[u]["X"] = eye - st[u]["L"] * lev
    s = 2
    while s < CHUNK:
        lev = ((i // (2 * s)) == (j // (2 * s))) & ((i // s) > (j // s))
        for u in units:
            x = st[u]["X"]
            xb = x.astype(BF)
            c = jnp.where(lev, st[u]["L"], 0.0).astype(BF)
            y = mm(xb, c).astype(BF)
            st[u]["X"] = x - mm(y, xb)
        s *= 2
    maps = {}
    for u in units:
        t = st[u]
        c, p = u
        rhs = jnp.concatenate([t["nqb"], t["av"].astype(BF)], axis=1)
        wu = mm(t["X"].astype(BF), rhs)
        f = mm(t["arb"], wu.astype(BF))
        mid = mids[c][:, p * 128 : (p + 1) * 128]
        end = ends[c][:, p * 128 : (p + 1) * 128]
        emid = jnp.exp(mid)
        q = fold(t["rqb"].astype(F32) - f[:, :128]) * emid
        o = fold(t["ov"] - f[:, 128:])
        rows = slice(c * CHUNK, (c + 1) * CHUNK)
        q_ref[rows, p * 128 : (p + 1) * 128] = q.astype(BF)
        o_ref[rows, p * 128 : (p + 1) * 128] = o
        w1 = fold(wu[:, :128])
        u0 = fold(wu[:, 128:])
        tail = jnp.exp(end - mid)
        left = jnp.concatenate([cut(kk, u) * tail, cut(bb, u) * tail], axis=0).T.astype(BF)
        right = jnp.concatenate(
            [
                jnp.concatenate([t["vb"].astype(F32), jnp.zeros((64, 128), F32)], axis=1),
                jnp.concatenate([-u0, w1], axis=1),
            ],
            axis=0,
        ).astype(BF)
        be = mm(left, right)
        m = jnp.where(i == j, jnp.exp(end), 0.0) - jnp.where(bd, be[:, 128:], 0.0) * emid
        bm = jnp.where(bd, be[:, :128], 0.0)
        maps[u] = (m, bm)
        mc_ref[step * GROUP + c, p] = m
        bc_ref[step * GROUP + c, p] = bm
    for p in range(2):
        lo = compose(maps[(0, p)], maps[(1, p)])
        hi = compose(maps[(2, p)], maps[(3, p)])
        m, bm = compose(lo, hi)
        mg_ref[step, p] = m
        bg_ref[step, p] = bm

    @pl.when(step == pl.num_programs(0) - 1)
    def _():
        for p in range(2):
            lo = compose((mg_ref[0, p], bg_ref[0, p]), (mg_ref[1, p], bg_ref[1, p]))
            hi = compose((mg_ref[2, p], bg_ref[2, p]), (mg_ref[3, p], bg_ref[3, p]))
            m, bm = compose(lo, hi)
            pk_ref[p] = pack_map(m, bm)


def chunk_maps(r, k, v, d, a, x):
    tokens, width = r.shape
    steps = tokens // ROWS
    chunks = tokens // CHUNK
    blk = pl.BlockSpec((ROWS, width), lambda s: (s, 0))
    whole = lambda shape: pl.BlockSpec(shape, lambda s: (0,) * len(shape))
    shapes = [
        jax.ShapeDtypeStruct((tokens, width), BF),
        jax.ShapeDtypeStruct((tokens, width), F32),
        jax.ShapeDtypeStruct((chunks, 2, 128, 128), F32),
        jax.ShapeDtypeStruct((chunks, 2, 128, 128), F32),
        jax.ShapeDtypeStruct((steps, 2, 128, 128), F32),
        jax.ShapeDtypeStruct((steps, 2, 128, 128), F32),
        jax.ShapeDtypeStruct((2, 128, 128), BF),
    ]
    return pl.pallas_call(
        chunk_kernel,
        grid=(steps,),
        in_specs=[blk] * 6,
        out_specs=[blk, blk] + [whole(s.shape) for s in shapes[2:]],
        out_shape=shapes,
        compiler_params=pltpu.CompilerParams(dimension_semantics=("arbitrary",), vmem_limit_bytes=50 << 20),
        name="chunk_maps",
    )(r, k, v, d, a, x)


def stage_kernel(here_ref, g_ref, in_m_ref, in_b_ref, pk_ref):
    count = g_ref.shape[0]
    here = here_ref[0]
    i, j = iotas(128, 128)
    for p in range(2):
        total = unpack_map(g_ref[0, p])
        first = here > 0
        in_m = jnp.where(first, total[0], jnp.where(i == j, 1.0, 0.0))
        in_b = jnp.where(first, total[1], 0.0)
        for k in range(1, count):
            total = compose(total, unpack_map(g_ref[k, p]))
            passed = here > k
            in_m = jnp.where(passed, total[0], in_m)
            in_b = jnp.where(passed, total[1], in_b)
        in_m_ref[p] = in_m
        in_b_ref[p] = in_b
        pk_ref[p] = pack_map(total[0], total[1])


def stage(gathered, axis):
    here = lax.axis_index(axis).astype(jnp.int32).reshape(1)
    square = jax.ShapeDtypeStruct((2, 128, 128), F32)
    return pl.pallas_call(
        stage_kernel,
        in_specs=[pl.BlockSpec(memory_space=pltpu.SMEM), pl.BlockSpec(memory_space=pltpu.VMEM)],
        out_shape=[square, square, jax.ShapeDtypeStruct((2, 128, 128), BF)],
        name="stage",
    )(here, gathered)


def readout_kernel(
    here_ref, g_ref, my_ref, by_ref, mx_ref, bx_ref, q_ref, o_ref, mc_ref, bc_ref, mg_ref, bg_ref, gate_ref, gain_ref, out_ref, ps_ref
):
    steps = mg_ref.shape[0]
    tokens = q_ref.shape[0]
    here = here_ref[0]
    cur = [jnp.zeros((128, 128), F32)] * 2
    for k in range(g_ref.shape[0] - 1):
        for p in range(2):
            m, b = unpack_map(g_ref[k, p])
            cur[p] = jnp.where(here > k, b if k == 0 else mm3(m, cur[p]) + b, cur[p])
    cur = [mm3(my_ref[p], cur[p]) + by_ref[p] for p in range(2)]
    cur = [mm3(mx_ref[p], cur[p]) + bx_ref[p] for p in range(2)]
    for g in range(steps):
        for p in range(2):
            ps_ref[g * GROUP, p] = cur[p]
            if g + 1 < steps:
                cur[p] = mm3(mg_ref[g, p], cur[p]) + bg_ref[g, p]
    for c in range(GROUP - 1):
        for g in range(steps):
            for p in range(2):
                at = g * GROUP + c
                ps_ref[at + 1, p] = mm3(mc_ref[at, p], ps_ref[at, p]) + bc_ref[at, p]
    ones = head_ones(256)
    for c in range(tokens // CHUNK):
        rows = slice(c * CHUNK, (c + 1) * CHUNK)
        parts = [mm(q_ref[rows, p * 128 : (p + 1) * 128], ps_ref[c, p].astype(BF)) for p in range(2)]
        o = o_ref[rows] + jnp.concatenate(parts, axis=1)
        cen = o - head_sum(o, ones) * (1.0 / 64)
        var = head_sum(cen * cen, ones) * (1.0 / 64)
        y = cen * lax.rsqrt(var + 0.00064) * gain_ref[...] * gate_ref[rows].astype(F32)
        out_ref[rows] = y.astype(BF)


def readout(gathered, axis, maps, q, o, mc, bc, mg, bg, gate, gain):
    tokens, width = q.shape
    here = lax.axis_index(axis).astype(jnp.int32).reshape(1)
    vmem = pl.BlockSpec(memory_space=pltpu.VMEM)
    return pl.pallas_call(
        readout_kernel,
        in_specs=[pl.BlockSpec(memory_space=pltpu.SMEM)] + [vmem] * 13,
        out_shape=jax.ShapeDtypeStruct((tokens, width), BF),
        scratch_shapes=[pltpu.VMEM((tokens // CHUNK, 2, 128, 128), F32)],
        compiler_params=pltpu.CompilerParams(vmem_limit_bytes=50 << 20),
        name="readout",
    )(here, gathered, *maps, q, o, mc, bc, mg, bg, gate, gain.reshape(1, width))


def project_kernel(x_ref, m0, m1, m2, m3, w0, w1, w2, w3, r0, r1, r2, r3, gain_ref, normed_ref, stream_ref):
    step = pl.program_id(0)

    def work(r_ref):
        total = jnp.zeros(r_ref.shape, F32)
        for m, w in ((m0, w0), (m1, w1), (m2, w2), (m3, w3)):
            total = total + mm(m[...], w[...]).astype(BF).astype(F32)
        stream = (r_ref[...].astype(F32) + total).astype(BF)
        wide = stream.astype(F32)
        scale = lax.rsqrt(jnp.mean(wide * wide, axis=-1, keepdims=True) + 1e-6)
        normed_ref[...] = (wide * scale * gain_ref[...]).astype(BF)
        return stream

    for at, r_ref in enumerate((r0, r1, r2)):

        @pl.when(step == at + 1)
        def _(r_ref=r_ref):
            work(r_ref)

    @pl.when(step == 0)
    def _():
        stream_ref[...] = work(r3)


def project(x, mixed, weights, rows, gain):
    tokens, width = mixed[0].shape
    depth = weights[0].shape[1]
    quarter = rows[0].shape[0]
    by_step = pl.BlockSpec((quarter, width), lambda s, x: ((x[0] + s) % 4, 0))
    fixed = lambda shape: pl.BlockSpec(shape, lambda s, x: (0, 0))
    return pl.pallas_call(
        project_kernel,
        grid_spec=pltpu.PrefetchScalarGridSpec(
            num_scalar_prefetch=1,
            grid=(4,),
            in_specs=[by_step] * 4 + [fixed((width, depth))] * 4 + [fixed((quarter, depth))] * 4 + [fixed((1, depth))],
            out_specs=[pl.BlockSpec((quarter, depth), lambda s, x: ((x[0] + s) % 4, 0)), fixed((quarter, depth))],
        ),
        out_shape=[jax.ShapeDtypeStruct((tokens, depth), BF), jax.ShapeDtypeStruct((quarter, depth), BF)],
        compiler_params=pltpu.CompilerParams(dimension_semantics=("arbitrary",), vmem_limit_bytes=56 << 20),
        name="project",
    )(x, *mixed, *weights, *rows, gain.reshape(1, depth))


HALO = 16
UNITS = 128
COLS = 256


def feed_kernel(offsets, first_steps, x_ref, *refs):
    n = len(offsets)
    blocks, halos = refs[:n], refs[n : 2 * n]
    edge_ref, gu_ref, down_ref, taps_ref = refs[2 * n : 2 * n + 4]
    out_ref, rows_ref, hidden_ref = refs[2 * n + 4 :]
    quarter = blocks[0].shape[0]
    each = quarter + HALO
    step = pl.program_id(0)

    @pl.when(step == 0)
    def _():
        for a in range(n):
            q = (x_ref[0] + offsets[a]) % 4
            rows_ref[a * each : a * each + HALO] = jnp.where(q == 0, edge_ref[...], halos[a][...])
            rows_ref[a * each + HALO : (a + 1) * each] = blocks[a][...]

    @pl.when(step < first_steps)
    def _():
        pre = mm(rows_ref[...], gu_ref[...]).astype(BF).astype(F32)
        taps = taps_ref[...]
        mix = taps[0:1] * pltpu.roll(pre, 2, 0) + taps[1:2] * pltpu.roll(pre, 1, 0) + taps[2:3] * pre
        gate = mix[:, :UNITS]
        hid = (gate / (1.0 + jnp.exp(-gate)) * mix[:, UNITS:]).astype(BF)
        for a in range(n):
            hidden_ref[step, a * quarter : (a + 1) * quarter] = hid[a * each + HALO : (a + 1) * each]

    @pl.when(step >= first_steps)
    def _():
        hid = jnp.concatenate([hidden_ref[f] for f in range(first_steps)], axis=1)
        part = mm_nt(hid, down_ref[...]).astype(BF)
        for a in range(n):
            out_ref[a, 0] = part[a * quarter : (a + 1) * quarter]


def feed(offsets, x, normed, edge, weights, taps):
    tokens, depth = normed.shape
    quarter = tokens // 4
    n = len(offsets)
    width = weights.shape[1] // 3
    first_steps = width // UNITS
    second_steps = depth // COLS
    half_steps = second_steps // 2
    last = first_steps - 1

    def block_of(off):
        return pl.BlockSpec((quarter, depth), lambda s, x: ((x[0] + off) % 4, 0))

    def halo_of(off):
        per = quarter // HALO
        return pl.BlockSpec((HALO, depth), lambda s, x: (jnp.maximum((x[0] + off) % 4 * per - 1, 0), 0))

    def out_at(s, x):
        at = jnp.maximum(s - first_steps, 0)
        return (0, at // half_steps, 0, at % half_steps)

    return pl.pallas_call(
        lambda *refs: feed_kernel(offsets, first_steps, *refs),
        grid_spec=pltpu.PrefetchScalarGridSpec(
            num_scalar_prefetch=1,
            grid=(first_steps + second_steps,),
            in_specs=[block_of(o) for o in offsets]
            + [halo_of(o) for o in offsets]
            + [
                pl.BlockSpec((HALO, depth), lambda s, x: (0, 0)),
                pl.BlockSpec((depth, 2 * UNITS), lambda s, x: (0, jnp.minimum(s, last))),
                pl.BlockSpec((COLS, width), lambda s, x: (jnp.maximum(s - first_steps, 0), 2)),
                pl.BlockSpec((8, 2 * UNITS), lambda s, x: (0, jnp.minimum(s, last))),
            ],
            out_specs=pl.BlockSpec((n, 1, quarter, COLS), out_at),
            scratch_shapes=[
                pltpu.VMEM((n * (quarter + HALO), depth), BF),
                pltpu.VMEM((first_steps, n * quarter, UNITS), BF),
            ],
        ),
        out_shape=jax.ShapeDtypeStruct((n, 2, quarter, depth // 2), BF),
        compiler_params=pltpu.CompilerParams(dimension_semantics=("arbitrary",), vmem_limit_bytes=56 << 20),
        name="feed",
    )(x, *([normed] * n), *([normed] * n), edge, weights, weights, taps)


def shifted(x, by):
    n = lax.axis_size("tp")
    return lax.ppermute(x, "tp", [(i, (i + by) % n) for i in range(n)])


def around(x):
    half = x.shape[0] // 2
    left = shifted(x, 1)
    right = shifted(x, -1)
    far = jnp.concatenate([shifted(left[:half], 1), shifted(right[half:], -1)], axis=0)
    return right, far, left


def passed_along(x, axis, by):
    count = lax.axis_size(axis)
    pairs = [(i, i + by) for i in range(count) if 0 <= i + by < count]
    return lax.ppermute(x, axis, pairs)


def side_by_side(a, b):
    lead = a.shape[:-1]
    cut = lambda t: t.reshape(*lead, -1, 1, UNITS)
    return jnp.concatenate([cut(a), cut(b)], axis=-2).reshape(*lead, 2 * a.shape[-1])


def body(
    residual_input_stream,
    receptance,
    key_matrix_all,
    value_matrix_all,
    decay_preactivation,
    learning_rate_preactivation,
    output_gate_all_heads,
    extra_log_decay,
    head_norm_gain,
    output_projection_weight,
    feedforward_norm_gain,
    gate_projection_weight,
    up_projection_weight,
    down_projection_weight,
    convolution_kernel,
):
    x = lax.axis_index("tp").astype(jnp.int32).reshape(1)
    local = jnp.concatenate(
        [side_by_side(gate_projection_weight, up_projection_weight), down_projection_weight], axis=1
    )
    weights = lax.all_gather(local, SP, axis=0, tiled=True)
    taps = side_by_side(convolution_kernel[:, 0], convolution_kernel[:, 1]).astype(F32)
    taps = jnp.concatenate([taps, jnp.zeros((5, taps.shape[1]), F32)], axis=0)

    row_pieces = around(residual_input_stream)
    proj_pieces = around(output_projection_weight)

    q, o, mc, bc, mg, bg, pk = chunk_maps(
        receptance,
        key_matrix_all,
        value_matrix_all,
        decay_preactivation,
        learning_rate_preactivation,
        extra_log_decay,
    )
    mx, bx, pk = stage(lax.all_gather(pk, "sp_2"), "sp_2")
    my, by, pk = stage(lax.all_gather(pk, "sp_1"), "sp_1")
    mixed = readout(
        lax.all_gather(pk, "sp_0"), "sp_0", (my, by, mx, bx), q, o, mc, bc, mg, bg, output_gate_all_heads, head_norm_gain
    )
    mixed_pieces = around(mixed)
    normed, stream = project(
        x,
        (*mixed_pieces, mixed),
        (*proj_pieces, output_projection_weight),
        (*row_pieces, residual_input_stream),
        feedforward_norm_gain,
    )
    edge = passed_along(normed[-HALO:], SP, 1)
    far = feed((2,), x, normed, edge, weights, taps)[0]
    to_right = shifted(far[0], 1)
    to_left = shifted(far[1], -1)
    near = feed((1, 3), x, normed, edge, weights, taps)
    got_right_b = shifted(near[0, 1], 1)
    got_left_a = shifted(near[1, 0], -1)
    add = lambda a, b: (a.astype(F32) + b.astype(F32)).astype(BF)
    got_right_a = shifted(add(near[0, 0], to_right), 1)
    got_left_b = shifted(add(near[1, 1], to_left), -1)
    own = feed((0,), x, normed, edge, weights, taps)[0]
    wide = lambda t: t.astype(F32)
    half_a = wide(own[0]) + wide(got_right_a) + wide(got_left_a)
    half_b = wide(own[1]) + wide(got_right_b) + wide(got_left_b)
    return (wide(stream) + jnp.concatenate([half_a, half_b], axis=1)).astype(BF)


def solution(mesh):
    split = Mesh(mesh.devices.reshape(4, 4, 2, mesh.shape["tp"]), ("sp_0", "sp_1", "sp_2", "tp"))
    in_specs = (
        P(SP_TP, None),
        P(SP, "tp"),
        P(SP, "tp"),
        P(SP, "tp"),
        P(SP, "tp"),
        P(SP, "tp"),
        P(SP, "tp"),
        P(SP, "tp"),
        P("tp"),
        P("tp", None),
        P(),
        P(SP, "tp"),
        P(SP, "tp"),
        P(SP, "tp"),
        P(None, None, "tp"),
    )
    out_specs = P(SP_TP, None)
    return jax.shard_map(body, mesh=split, in_specs=in_specs, out_specs=out_specs, check_vma=False)
```

```python
import jax
import jax.numpy as jnp
from jax import lax
from jax.experimental import pallas as pl
from jax.experimental.pallas import tpu as pltpu
from jax.sharding import Mesh
from jax.sharding import PartitionSpec as P

SP = ("sp_0", "sp_1", "sp_2")
SP_TP = ("sp_0", "sp_1", "sp_2", "tp")

BF = jnp.bfloat16
F32 = jnp.float32
CHUNK = 64
GROUP = 4
ROWS = CHUNK * GROUP


def in_hbm(x):
    return pltpu.with_memory_space_constraint(x, pltpu.HBM)


def in_vmem(x):
    return pltpu.with_memory_space_constraint(x, pltpu.VMEM)


def whole(shape):
    return pl.BlockSpec(tuple(shape), lambda *_: (0,) * len(shape))


def mm(a, b):
    return lax.dot_general(a, b, (((1,), (0,)), ((), ())), preferred_element_type=F32)


def mm_nt(a, b):
    return lax.dot_general(a, b, (((1,), (1,)), ((), ())), preferred_element_type=F32)


def split2(x):
    hi = x.astype(BF)
    return hi, (x - hi.astype(F32)).astype(BF)


def mm3(a, b):
    ah, al = split2(a)
    bh, bl = split2(b)
    return mm(ah, bh) + (mm(ah, bl) + mm(al, bh))


def iotas(n, m):
    return lax.broadcasted_iota(jnp.int32, (n, m), 0), lax.broadcasted_iota(jnp.int32, (n, m), 1)


def head_ones(n):
    i, j = iotas(n, n)
    return jnp.where((i // 64) == (j // 64), 1.0, 0.0).astype(BF)


def head_sum(x, ones):
    hi, lo = split2(x)
    return mm(hi, ones) + mm(lo, ones)


def block_diagonal(n):
    i, j = iotas(n, n)
    return (i // 64) == (j // 64)


def pack_map(m, b):
    i, j = iotas(128, 128)
    e = m - jnp.where(i == j, 1.0, 0.0)
    return jnp.where(j < 64, e + pltpu.roll(e, 64, 1), b + pltpu.roll(b, 64, 1)).astype(BF)


def unpack_map(p):
    i, j = iotas(128, 128)
    p = p.astype(F32)
    s = pltpu.roll(p, 64, 1)
    bd = (i // 64) == (j // 64)
    m = jnp.where(bd, jnp.where(j < 64, p, s), 0.0) + jnp.where(i == j, 1.0, 0.0)
    b = jnp.where(bd, jnp.where(j < 64, s, p), 0.0)
    return m, b


def compose(first, second):
    both = mm3(second[0], jnp.concatenate([first[0], first[1]], axis=1))
    return both[:, :128], both[:, 128:] + second[1]


def chunk_kernel(r_ref, k_ref, v_ref, d_ref, a_ref, x_ref, q_ref, o_ref, pc_ref, mg_ref, bg_ref, pk_ref):
    step = pl.program_id(0)
    ones = head_ones(256)
    k = k_ref[...].astype(F32)
    n = k * lax.rsqrt(head_sum(k * k, ones) + 1e-6)
    rate = 1.0 / (1.0 + jnp.exp(-a_ref[...].astype(F32)))
    b = n * rate
    ld = (-0.6065306597126334) / (1.0 + jnp.exp(-d_ref[...].astype(F32))) + x_ref[...]
    i, j = iotas(ROWS, ROWS)
    tri = jnp.where(((i // CHUNK) == (j // CHUNK)) & (i >= j), 1.0, 0.0).astype(BF)
    ldh, ldl = split2(ld)
    g = mm(tri, ldh) + mm(tri, ldl)
    mids = [g[c * CHUNK + CHUNK // 2 : c * CHUNK + CHUNK // 2 + 1] for c in range(GROUP)]
    ends = [g[c * CHUNK + CHUNK - 1 : c * CHUNK + CHUNK] for c in range(GROUP)]
    rel = jnp.concatenate([g[c * CHUNK : (c + 1) * CHUNK] - mids[c] for c in range(GROUP)], axis=0)
    up = jnp.exp(rel)
    prev = jnp.exp(rel - ld)
    down = jnp.exp(-rel)
    rq = r_ref[...].astype(F32) * up
    nq = n * prev
    kk = k * down
    bb = b * down
    v = v_ref[...]

    i, j = iotas(128, 128)
    bd = (i // 64) == (j // 64)
    ti, tj = i % 64, j % 64
    strict = bd & (ti > tj)
    within = bd & (ti >= tj)
    eye = jnp.where(i == j, 1.0, 0.0)
    mask_a = jnp.concatenate([jnp.concatenate([strict, strict], axis=1), jnp.concatenate([within, within], axis=1)], axis=0)
    low = lax.broadcasted_iota(jnp.int32, (64, 128), 1) < 64
    zero = jnp.zeros((64, 128), BF)

    def spread(x):
        return jnp.concatenate([jnp.where(low, x, zero), jnp.where(low, zero, x)], axis=0)

    def fold(x):
        return jnp.where(low, x[:64], x[64:])

    units = [(c, p) for c in range(GROUP) for p in range(2)]

    def cut(x, u):
        c, p = u
        return x[c * CHUNK : (c + 1) * CHUNK, p * 128 : (p + 1) * 128]

    st = {}
    for u in units:
        nqb = spread(cut(nq, u).astype(BF))
        rqb = spread(cut(rq, u).astype(BF))
        kb = cut(kk, u).astype(BF)
        bbb = cut(bb, u).astype(BF)
        vb = cut(v, u)
        vs = spread(vb)
        att = mm_nt(jnp.concatenate([nqb, rqb], axis=0), jnp.concatenate([kb, kb, bbb, bbb], axis=0))
        att = jnp.where(mask_a, att, 0.0)
        kv = mm(att[:, :128].astype(BF), vs)
        st[u] = dict(nqb=nqb, rqb=rqb, vb=vb, L=att[:128, 128:], arb=att[128:, 128:].astype(BF), av=kv[:128], ov=kv[128:])
    lev = jnp.where(bd & ((ti // 2) == (tj // 2)), 1.0, 0.0)
    for u in units:
        st[u]["X"] = eye - st[u]["L"] * lev
    s = 2
    while s < CHUNK:
        lev = ((i // (2 * s)) == (j // (2 * s))) & ((i // s) > (j // s))
        for u in units:
            x = st[u]["X"]
            xb = x.astype(BF)
            c = jnp.where(lev, st[u]["L"], 0.0).astype(BF)
            y = mm(xb, c).astype(BF)
            st[u]["X"] = x - mm(y, xb)
        s *= 2
    maps = {}
    for u in units:
        t = st[u]
        c, p = u
        rhs = jnp.concatenate([t["nqb"], t["av"].astype(BF)], axis=1)
        wu = mm(t["X"].astype(BF), rhs)
        f = mm(t["arb"], wu.astype(BF))
        mid = mids[c][:, p * 128 : (p + 1) * 128]
        end = ends[c][:, p * 128 : (p + 1) * 128]
        emid = jnp.exp(mid)
        q = fold(t["rqb"].astype(F32) - f[:, :128]) * emid
        o = fold(t["ov"] - f[:, 128:])
        rows = slice(c * CHUNK, (c + 1) * CHUNK)
        q_ref[rows, p * 128 : (p + 1) * 128] = q.astype(BF)
        o_ref[rows, p * 128 : (p + 1) * 128] = o
        w1 = fold(wu[:, :128])
        u0 = fold(wu[:, 128:])
        tail = jnp.exp(end - mid)
        left = jnp.concatenate([cut(kk, u) * tail, cut(bb, u) * tail], axis=0).T.astype(BF)
        right = jnp.concatenate(
            [
                jnp.concatenate([t["vb"].astype(F32), jnp.zeros((64, 128), F32)], axis=1),
                jnp.concatenate([-u0, w1], axis=1),
            ],
            axis=0,
        ).astype(BF)
        be = mm(left, right)
        m = jnp.where(i == j, jnp.exp(end), 0.0) - jnp.where(bd, be[:, 128:], 0.0) * emid
        bm = jnp.where(bd, be[:, :128], 0.0)
        maps[u] = (m, bm)
        pc_ref[step * GROUP + c, p] = pack_map(m, bm)
    for p in range(2):
        lo = compose(maps[(0, p)], maps[(1, p)])
        hi = compose(maps[(2, p)], maps[(3, p)])
        m, bm = compose(lo, hi)
        mg_ref[step, p] = m
        bg_ref[step, p] = bm

    @pl.when(step == pl.num_programs(0) - 1)
    def _():
        for p in range(2):
            lo = compose((mg_ref[0, p], bg_ref[0, p]), (mg_ref[1, p], bg_ref[1, p]))
            hi = compose((mg_ref[2, p], bg_ref[2, p]), (mg_ref[3, p], bg_ref[3, p]))
            m, bm = compose(lo, hi)
            pk_ref[p] = pack_map(m, bm)


def chunk_maps(r, k, v, d, a, x):
    tokens, width = r.shape
    steps = tokens // ROWS
    chunks = tokens // CHUNK
    blk = pl.BlockSpec((ROWS, width), lambda s: (s, 0))
    shapes = [
        pltpu.HBM((tokens, width), BF),
        pltpu.HBM((tokens, width), F32),
        pltpu.HBM((chunks, 2, 128, 128), BF),
        pltpu.HBM((steps, 2, 128, 128), F32),
        pltpu.HBM((steps, 2, 128, 128), F32),
        pltpu.VMEM((2, 128, 128), BF),
    ]
    return pl.pallas_call(
        chunk_kernel,
        grid=(steps,),
        in_specs=[blk] * 6,
        out_specs=[blk, blk] + [whole(s.shape) for s in shapes[2:5]] + [pl.BlockSpec(memory_space=pltpu.VMEM)],
        out_shape=shapes,
        compiler_params=pltpu.CompilerParams(dimension_semantics=("arbitrary",), vmem_limit_bytes=16 << 20),
        name="chunk_maps",
    )(*map(in_hbm, (r, k, v, d, a, x)))


def stage_kernel(count, here_ref, *refs):
    in_m_ref, in_b_ref, pk_ref, g_ref = refs[count:]
    here = here_ref[0]
    for k in range(count):
        g_ref[(here + count - k) % count] = refs[k][...]
    i, j = iotas(128, 128)
    for p in range(2):
        total = unpack_map(g_ref[0, p])
        first = here > 0
        in_m = jnp.where(first, total[0], jnp.where(i == j, 1.0, 0.0))
        in_b = jnp.where(first, total[1], 0.0)
        for k in range(1, count):
            total = compose(total, unpack_map(g_ref[k, p]))
            passed = here > k
            in_m = jnp.where(passed, total[0], in_m)
            in_b = jnp.where(passed, total[1], in_b)
        in_m_ref[p] = in_m
        in_b_ref[p] = in_b
        pk_ref[p] = pack_map(total[0], total[1])


def stage(gathered, axis):
    here = lax.axis_index(axis).astype(jnp.int32).reshape(1)
    square = pltpu.VMEM((2, 128, 128), F32)
    count = len(gathered)
    vmem = pl.BlockSpec(memory_space=pltpu.VMEM)
    return pl.pallas_call(
        lambda *refs: stage_kernel(count, *refs),
        in_specs=[pl.BlockSpec(memory_space=pltpu.SMEM)] + [vmem] * count,
        out_specs=[vmem] * 3,
        out_shape=[square, square, pltpu.VMEM((2, 128, 128), BF)],
        scratch_shapes=[pltpu.VMEM((count, 2, 128, 128), BF)],
        compiler_params=pltpu.CompilerParams(vmem_limit_bytes=4 << 20),
        name="stage",
    )(here, *map(in_vmem, gathered))


def advance(packed, state):
    i, j = iotas(128, 128)
    packed = packed.astype(F32)
    other = pltpu.roll(packed, 64, 1)
    bd = (i // 64) == (j // 64)
    e = jnp.where(bd, jnp.where(j < 64, packed, other), 0.0).astype(BF)
    b = jnp.where(bd, jnp.where(j < 64, other, packed), 0.0)
    hi, lo = split2(state)
    return state + (mm(e, hi) + mm(e, lo)) + b


def readout_kernel(count, here_ref, *refs):
    my_ref, by_ref, mx_ref, bx_ref, q_ref, o_ref, pc_ref, mg_ref, bg_ref, gate_ref, gain_ref, out_ref, ps_ref, g_ref = refs[count:]
    steps = mg_ref.shape[0]
    tokens = q_ref.shape[0]
    here = here_ref[0]
    for k in range(count):
        g_ref[(here + count - k) % count] = refs[k][...]
    cur = [jnp.zeros((128, 128), F32)] * 2
    for k in range(g_ref.shape[0] - 1):
        for p in range(2):
            m, b = unpack_map(g_ref[k, p])
            cur[p] = jnp.where(here > k, b if k == 0 else mm3(m, cur[p]) + b, cur[p])
    cur = [mm3(my_ref[p], cur[p]) + by_ref[p] for p in range(2)]
    cur = [mm3(mx_ref[p], cur[p]) + bx_ref[p] for p in range(2)]
    for g in range(steps):
        for p in range(2):
            ps_ref[g * GROUP, p] = cur[p]
            if g + 1 < steps:
                cur[p] = mm3(mg_ref[g, p], cur[p]) + bg_ref[g, p]
    for c in range(GROUP - 1):
        for g in range(steps):
            for p in range(2):
                at = g * GROUP + c
                ps_ref[at + 1, p] = advance(pc_ref[at, p], ps_ref[at, p])
    ones = head_ones(256)
    for c in range(tokens // CHUNK):
        rows = slice(c * CHUNK, (c + 1) * CHUNK)
        parts = [mm(q_ref[rows, p * 128 : (p + 1) * 128], ps_ref[c, p].astype(BF)) for p in range(2)]
        o = o_ref[rows] + jnp.concatenate(parts, axis=1)
        cen = o - head_sum(o, ones) * (1.0 / 64)
        var = head_sum(cen * cen, ones) * (1.0 / 64)
        y = cen * lax.rsqrt(var + 0.00064) * gain_ref[...] * gate_ref[rows].astype(F32)
        out_ref[rows] = y.astype(BF)


def readout(gathered, axis, maps, q, o, pc, mg, bg, gate, gain):
    tokens, width = q.shape
    here = lax.axis_index(axis).astype(jnp.int32).reshape(1)
    count = len(gathered)
    near = (*gathered, *maps)
    far = (q, o, pc, mg, bg, gate, gain.reshape(1, width))
    vmem = pl.BlockSpec(memory_space=pltpu.VMEM)
    return pl.pallas_call(
        lambda *refs: readout_kernel(count, *refs),
        grid=(1,),
        in_specs=[pl.BlockSpec(memory_space=pltpu.SMEM)] + [vmem] * len(near) + [whole(a.shape) for a in far],
        out_specs=vmem,
        out_shape=pltpu.VMEM((tokens, width), BF),
        scratch_shapes=[pltpu.VMEM((tokens // CHUNK, 2, 128, 128), F32), pltpu.VMEM((count, 2, 128, 128), BF)],
        compiler_params=pltpu.CompilerParams(vmem_limit_bytes=16 << 20),
        name="readout",
    )(here, *map(in_vmem, near), *map(in_hbm, far))


def project_kernel(x_ref, *refs):
    m_own, m_right, m_far_a, m_far_b, m_left, w_right, w_far, w_left, r_right, r_far, r_left, gain_ref = refs[:12]
    w_hbm, r_hbm, weights_ref, normed_ref, stream_ref, held_ref, w_own, r_own, sems = refs[12:]
    quarter, depth = stream_ref.shape
    span = weights_ref.shape[0] // 8
    moves = [(w_hbm, w_own), (r_hbm, r_own)]
    moves += [(weights_ref.at[pl.ds(c * span, span)], held_ref.at[pl.ds(c * span, span)]) for c in range(8)]
    copies = [pltpu.make_async_copy(a, b, sems.at[i]) for i, (a, b) in enumerate(moves)]
    for c in copies:
        c.start()
    copies[0].wait()
    for s, rows in ((1, r_right), (2, r_far), (3, r_left), (0, r_own)):
        if s == 0:
            copies[1].wait()
        q = (x_ref[0] + s) % 4
        at = pl.multiple_of(q * quarter, quarter)
        low = pl.multiple_of(jnp.minimum(q, 1) * quarter, quarter)
        high = pl.multiple_of(jnp.maximum(q - 2, 0) * quarter, quarter)
        m_far = jnp.where(q < 2, m_far_a[pl.ds(low, quarter)], m_far_b[pl.ds(high, quarter)])
        part = mm(m_own[pl.ds(at, quarter)], w_own[...]) + mm(m_right[pl.ds(at, quarter)], w_right[...])
        part = part + mm(m_far, w_far[...]) + mm(m_left[pl.ds(at, quarter)], w_left[...])
        stream = (rows[...].astype(F32) + part).astype(BF)
        wide = stream.astype(F32)
        scale = lax.rsqrt(jnp.mean(wide * wide, axis=-1, keepdims=True) + 1e-6)
        normed_ref[pl.ds(at, quarter)] = (wide * scale * gain_ref[...]).astype(BF)
        if s == 0:
            stream_ref[...] = stream
    for c in copies[2:]:
        c.wait()


def project(x, mixed, projs, rows, weights, gain):
    tokens, width = mixed[0].shape
    quarter, depth = rows[0].shape
    any_space = pl.BlockSpec(memory_space=pltpu.HBM)
    vmem = pl.BlockSpec(memory_space=pltpu.VMEM)
    near = [*mixed, *projs[1:], *rows[1:], gain.reshape(1, depth)]
    return pl.pallas_call(
        project_kernel,
        in_specs=[pl.BlockSpec(memory_space=pltpu.SMEM)] + [vmem] * len(near) + [any_space] * 3,
        out_specs=[vmem, vmem, vmem],
        out_shape=[
            pltpu.VMEM((tokens, depth), BF),
            pltpu.VMEM((quarter, depth), BF),
            pltpu.VMEM(weights.shape, BF),
        ],
        scratch_shapes=[pltpu.VMEM((width, depth), BF), pltpu.VMEM((quarter, depth), BF), pltpu.SemaphoreType.DMA((10,))],
        compiler_params=pltpu.CompilerParams(vmem_limit_bytes=12 << 20),
        name="project",
    )(x, *map(in_vmem, near), projs[0], rows[0], weights)


HALO = 16
COLS = 256


def feed_kernel(offset, x_ref, normed_ref, edge_ref, w_ref, taps_ref, a_ref, b_ref, rows_ref, hidden_ref, pre_ref):
    quarter, half = a_ref.shape
    width = hidden_ref.shape[1]
    steps = width // COLS
    rest = width - steps * COLS
    q = (x_ref[0] + offset) % 4
    before = pl.multiple_of(jnp.maximum(q * quarter - HALO, 0), HALO)
    rows_ref[:HALO] = jnp.where(q == 0, edge_ref[...], normed_ref[pl.ds(before, HALO)])
    rows_ref[HALO:] = normed_ref[pl.ds(pl.multiple_of(q * quarter, quarter), quarter)]

    def product(slot, at, count):
        rows = rows_ref[...]
        for side in range(2):
            cols = slice(side * width + at, side * width + at + count)
            pre_ref[slot, side, :, :count] = mm(rows, w_ref[:, cols]).astype(BF)

    def mixing(slot, at, count):
        mixes = []
        for side in range(2):
            pre = pre_ref[slot, side, :, :count].astype(F32)
            taps = taps_ref[side, :, at : at + count]
            mixes.append(taps[0:1] * pltpu.roll(pre, 2, 0) + taps[1:2] * pltpu.roll(pre, 1, 0) + taps[2:3] * pre)
        hid = (mixes[0] / (1.0 + jnp.exp(-mixes[0])) * mixes[1]).astype(BF)
        hidden_ref[:, at : at + count] = hid[HALO:]

    starts = [(f * COLS, COLS) for f in range(steps)] + ([(steps * COLS, rest)] if rest else [])
    for f, (at, count) in enumerate(starts):
        product(f % 2, at, count)
        if f:
            mixing((f - 1) % 2, *starts[f - 1])
    mixing((len(starts) - 1) % 2, *starts[-1])
    for h, out_ref in enumerate((a_ref, b_ref)):
        out_ref[...] = mm_nt(hidden_ref[...], w_ref[h * half : (h + 1) * half, 2 * width :]).astype(BF)


def feed(offset, x, normed, edge, weights, taps):
    tokens, depth = normed.shape
    quarter = tokens // 4
    width = weights.shape[1] // 3
    vmem = pl.BlockSpec(memory_space=pltpu.VMEM)
    return pl.pallas_call(
        lambda *refs: feed_kernel(offset, *refs),
        in_specs=[pl.BlockSpec(memory_space=pltpu.SMEM)] + [vmem] * 4,
        out_specs=[vmem, vmem],
        scratch_shapes=[
            pltpu.VMEM((quarter + HALO, depth), BF),
            pltpu.VMEM((quarter, width), BF),
            pltpu.VMEM((2, 2, quarter + HALO, COLS), BF),
        ],
        out_shape=[jax.ShapeDtypeStruct((quarter, depth // 2), BF)] * 2,
        compiler_params=pltpu.CompilerParams(vmem_limit_bytes=12 << 20),
        name="feed",
    )(x, in_vmem(normed), edge, in_vmem(weights), taps)


def shifted(x, by):
    n = lax.axis_size("tp")
    return lax.ppermute(x, "tp", [(i, (i + by) % n) for i in range(n)])


def passed_along(x, axis, by):
    count = lax.axis_size(axis)
    pairs = [(i, i + by) for i in range(count) if 0 <= i + by < count]
    return lax.ppermute(x, axis, pairs)


def everyone(x, axis):
    n = lax.axis_size(axis)
    return [x] + [lax.ppermute(x, axis, [(i, (i + by) % n) for i in range(n)]) for by in range(1, n)]


def body(
    residual_input_stream,
    receptance,
    key_matrix_all,
    value_matrix_all,
    decay_preactivation,
    learning_rate_preactivation,
    output_gate_all_heads,
    extra_log_decay,
    head_norm_gain,
    output_projection_weight,
    feedforward_norm_gain,
    gate_projection_weight,
    up_projection_weight,
    down_projection_weight,
    convolution_kernel,
):
    x = lax.axis_index("tp").astype(jnp.int32).reshape(1)
    local = jnp.concatenate([gate_projection_weight, up_projection_weight, down_projection_weight], axis=1)
    weights = lax.all_gather(local, SP, axis=0, tiled=True)
    taps = convolution_kernel.astype(F32).transpose(1, 0, 2)

    row_left, row_right = shifted(residual_input_stream, 1), shifted(residual_input_stream, -1)
    proj_left, proj_right = shifted(output_projection_weight, 1), shifted(output_projection_weight, -1)

    q, o, pc, mg, bg, pk = chunk_maps(
        receptance,
        key_matrix_all,
        value_matrix_all,
        decay_preactivation,
        learning_rate_preactivation,
        extra_log_decay,
    )
    mx, bx, pk = stage(everyone(pk, "sp_2"), "sp_2")
    my, by, pk = stage(everyone(pk, "sp_1"), "sp_1")
    pk, row_left, row_right, proj_left, proj_right = lax.optimization_barrier(
        (pk, row_left, row_right, proj_left, proj_right)
    )
    row_far, proj_far = shifted(row_left, 1), shifted(proj_right, -1)
    mixed = readout(
        everyone(pk, "sp_0"), "sp_0", (my, by, mx, bx), q, o, pc, mg, bg, output_gate_all_heads, head_norm_gain
    )
    mixed, row_far, proj_far = lax.optimization_barrier((mixed, row_far, proj_far))
    half = mixed.shape[0] // 2
    mixed_left, mixed_right = shifted(mixed, 1), shifted(mixed, -1)
    mixed_far = (shifted(mixed_left[:half], 1), shifted(mixed_right[half:], -1))
    normed, stream, weights = project(
        x,
        (mixed, mixed_right, *mixed_far, mixed_left),
        (output_projection_weight, proj_right, proj_far, proj_left),
        (residual_input_stream, row_right, row_far, row_left),
        weights,
        feedforward_norm_gain,
    )
    edge = passed_along(normed[-HALO:], SP, 1)
    add = lambda a, b: (a.astype(F32) + b.astype(F32)).astype(BF)
    far = feed(2, x, normed, edge, weights, taps)
    to_right = shifted(far[0], 1)
    to_left = shifted(far[1], -1)
    right = feed(1, x, normed, edge, weights, taps)
    got_right_b = shifted(right[1], 1)
    left = feed(3, x, normed, edge, weights, taps)
    got_left_a = shifted(left[0], -1)
    got_right_a = shifted(add(right[0], to_right), 1)
    got_left_b = shifted(add(left[1], to_left), -1)
    own = feed(0, x, normed, edge, weights, taps)
    wide = lambda t: t.astype(F32)
    half_a = wide(own[0]) + wide(got_right_a) + wide(got_left_a)
    half_b = wide(own[1]) + wide(got_right_b) + wide(got_left_b)
    return (wide(stream) + jnp.concatenate([half_a, half_b], axis=1)).astype(BF)


def solution(mesh):
    split = Mesh(mesh.devices.reshape(4, 4, 2, mesh.shape["tp"]), ("sp_0", "sp_1", "sp_2", "tp"))
    in_specs = (
        P(SP_TP, None),
        P(SP, "tp"),
        P(SP, "tp"),
        P(SP, "tp"),
        P(SP, "tp"),
        P(SP, "tp"),
        P(SP, "tp"),
        P(SP, "tp"),
        P("tp"),
        P("tp", None),
        P(),
        P(SP, "tp"),
        P(SP, "tp"),
        P(SP, "tp"),
        P(None, None, "tp"),
    )
    out_specs = P(SP_TP, None)
    return jax.shard_map(body, mesh=split, in_specs=in_specs, out_specs=out_specs, check_vma=False)
```

```python
import jax
import jax.numpy as jnp
from jax import lax
from jax.experimental import pallas as pl
from jax.experimental.pallas import tpu as pltpu
from jax.sharding import Mesh
from jax.sharding import PartitionSpec as P

SP = ("sp_0", "sp_1", "sp_2")
SP_TP = ("sp_0", "sp_1", "sp_2", "tp")

BF = jnp.bfloat16
F32 = jnp.float32
CHUNK = 64
GROUP = 4
ROWS = CHUNK * GROUP


def in_hbm(x):
    return pltpu.with_memory_space_constraint(x, pltpu.HBM)


def in_vmem(x):
    return pltpu.with_memory_space_constraint(x, pltpu.VMEM)


def whole(shape):
    return pl.BlockSpec(tuple(shape), lambda *_: (0,) * len(shape))


def mm(a, b):
    return lax.dot_general(a, b, (((1,), (0,)), ((), ())), preferred_element_type=F32)


def mm_nt(a, b):
    return lax.dot_general(a, b, (((1,), (1,)), ((), ())), preferred_element_type=F32)


def split2(x):
    hi = x.astype(BF)
    return hi, (x - hi.astype(F32)).astype(BF)


def mm3(a, b):
    ah, al = split2(a)
    bh, bl = split2(b)
    return mm(ah, bh) + (mm(ah, bl) + mm(al, bh))


def iotas(n, m):
    return lax.broadcasted_iota(jnp.int32, (n, m), 0), lax.broadcasted_iota(jnp.int32, (n, m), 1)


def head_ones(n):
    i, j = iotas(n, n)
    return jnp.where((i // 64) == (j // 64), 1.0, 0.0).astype(BF)


def head_sum(x, ones):
    hi, lo = split2(x)
    return mm(hi, ones) + mm(lo, ones)


def block_diagonal(n):
    i, j = iotas(n, n)
    return (i // 64) == (j // 64)


def pack_map(m, b):
    i, j = iotas(128, 128)
    e = m - jnp.where(i == j, 1.0, 0.0)
    return jnp.where(j < 64, e + pltpu.roll(e, 64, 1), b + pltpu.roll(b, 64, 1)).astype(BF)


def unpack_map(p):
    i, j = iotas(128, 128)
    p = p.astype(F32)
    s = pltpu.roll(p, 64, 1)
    bd = (i // 64) == (j // 64)
    m = jnp.where(bd, jnp.where(j < 64, p, s), 0.0) + jnp.where(i == j, 1.0, 0.0)
    b = jnp.where(bd, jnp.where(j < 64, s, p), 0.0)
    return m, b


def compose(first, second):
    both = mm3(second[0], jnp.concatenate([first[0], first[1]], axis=1))
    return both[:, :128], both[:, 128:] + second[1]


def tree(level):
    while len(level) > 1:
        level = [[compose(level[z][p], level[z + 1][p]) for p in range(2)] for z in range(0, len(level), 2)]
    return level[0]


def chunk_kernel(r_ref, k_ref, v_ref, d_ref, a_ref, x_ref, q_ref, o_ref, pc_ref, mg_ref, bg_ref, pk_ref):
    step = pl.program_id(0)
    ones = head_ones(256)
    k = k_ref[...].astype(F32)
    n = k * lax.rsqrt(head_sum(k * k, ones) + 1e-6)
    rate = 1.0 / (1.0 + jnp.exp(-a_ref[...].astype(F32)))
    b = n * rate
    ld = (-0.6065306597126334) / (1.0 + jnp.exp(-d_ref[...].astype(F32))) + x_ref[...]
    i, j = iotas(ROWS, ROWS)
    tri = jnp.where(((i // CHUNK) == (j // CHUNK)) & (i >= j), 1.0, 0.0).astype(BF)
    ldh, ldl = split2(ld)
    g = mm(tri, ldh) + mm(tri, ldl)
    mids = [g[c * CHUNK + CHUNK // 2 : c * CHUNK + CHUNK // 2 + 1] for c in range(GROUP)]
    ends = [g[c * CHUNK + CHUNK - 1 : c * CHUNK + CHUNK] for c in range(GROUP)]
    rel = jnp.concatenate([g[c * CHUNK : (c + 1) * CHUNK] - mids[c] for c in range(GROUP)], axis=0)
    up = jnp.exp(rel)
    prev = jnp.exp(rel - ld)
    down = jnp.exp(-rel)
    rq = r_ref[...].astype(F32) * up
    nq = n * prev
    kk = k * down
    bb = b * down
    v = v_ref[...]

    i, j = iotas(128, 128)
    bd = (i // 64) == (j // 64)
    ti, tj = i % 64, j % 64
    strict = bd & (ti > tj)
    within = bd & (ti >= tj)
    eye = jnp.where(i == j, 1.0, 0.0)
    mask_a = jnp.concatenate([jnp.concatenate([strict, strict], axis=1), jnp.concatenate([within, within], axis=1)], axis=0)
    low = lax.broadcasted_iota(jnp.int32, (64, 128), 1) < 64
    zero = jnp.zeros((64, 128), BF)

    def spread(x):
        return jnp.concatenate([jnp.where(low, x, zero), jnp.where(low, zero, x)], axis=0)

    def fold(x):
        return jnp.where(low, x[:64], x[64:])

    units = [(c, p) for c in range(GROUP) for p in range(2)]

    def cut(x, u):
        c, p = u
        return x[c * CHUNK : (c + 1) * CHUNK, p * 128 : (p + 1) * 128]

    st = {}
    for u in units:
        nqb = spread(cut(nq, u).astype(BF))
        rqb = spread(cut(rq, u).astype(BF))
        kb = cut(kk, u).astype(BF)
        bbb = cut(bb, u).astype(BF)
        vb = cut(v, u)
        att = mm_nt(jnp.concatenate([nqb, rqb], axis=0), jnp.concatenate([kb, kb, bbb, bbb], axis=0))
        st[u] = dict(nqb=nqb, rqb=rqb, vb=vb, att=att)
    for u in units:
        t = st[u]
        att = t.pop("att")
        t["L"] = jnp.where(strict, att[:128, 128:], 0.0)
        t["arb"] = jnp.where(within, att[128:, 128:], 0.0).astype(BF)
        t["ak"] = jnp.concatenate(
            [jnp.where(strict, att[:128, :128], 0.0).astype(BF), jnp.where(within, att[128:, :128], 0.0).astype(BF)], axis=0
        )
    lev = jnp.where(bd & ((ti // 2) == (tj // 2)), 1.0, 0.0)
    for u in units:
        st[u]["X"] = eye - st[u]["L"] * lev
    s = 2
    while s < CHUNK:
        lev = ((i // (2 * s)) == (j // (2 * s))) & ((i // s) > (j // s))
        for u in units:
            x = st[u]["X"]
            xb = x.astype(BF)
            c = jnp.where(lev, st[u]["L"], 0.0).astype(BF)
            y = mm(xb, c).astype(BF)
            st[u]["X"] = x - mm(y, xb)
        s *= 2
    for u in units:
        t = st[u]
        kv = mm(t["ak"], spread(t["vb"]))
        t["av"], t["ov"] = kv[:128].astype(BF), kv[128:]
    for u in units:
        t = st[u]
        t["wu"] = mm(t["X"].astype(BF), jnp.concatenate([t["nqb"], t["av"]], axis=1))
    for u in units:
        t = st[u]
        t["f"] = mm(t["arb"], t["wu"].astype(BF))
    for u in units:
        t = st[u]
        c, p = u
        wu = t["wu"]
        tail = jnp.exp(ends[c][:, p * 128 : (p + 1) * 128] - mids[c][:, p * 128 : (p + 1) * 128])
        left = jnp.concatenate([cut(kk, u) * tail, cut(bb, u) * tail], axis=0).T.astype(BF)
        right = jnp.concatenate(
            [
                jnp.concatenate([t["vb"], zero], axis=1),
                jnp.concatenate([-fold(wu[:, 128:]), fold(wu[:, :128])], axis=1).astype(BF),
            ],
            axis=0,
        )
        t["be"] = mm(left, right)
    maps = {}
    for u in units:
        t = st[u]
        c, p = u
        f = t["f"]
        lanes = slice(p * 128, (p + 1) * 128)
        emid = jnp.exp(mids[c][:, lanes])
        q = fold(t["rqb"].astype(F32) - f[:, :128]) * emid
        rows = slice(c * CHUNK, (c + 1) * CHUNK)
        q_ref[rows, lanes] = q.astype(BF)
        o_ref[rows, lanes] = fold(t["ov"] - f[:, 128:])
        be = t["be"]
        m = jnp.where(i == j, jnp.exp(ends[c][:, lanes]), 0.0) - jnp.where(bd, be[:, 128:], 0.0) * emid
        bm = jnp.where(bd, be[:, :128], 0.0)
        maps[u] = (m, bm)
        pc_ref[step * GROUP + c, p] = pack_map(m, bm)
    level = [[maps[(c, p)] for p in range(2)] for c in range(GROUP)]
    level = tree(level)
    for p in range(2):
        mg_ref[step, p], bg_ref[step, p] = level[p]

    @pl.when(step == pl.num_programs(0) - 1)
    def _():
        level = tree([[(mg_ref[z, p], bg_ref[z, p]) for p in range(2)] for z in range(mg_ref.shape[0])])
        for p in range(2):
            pk_ref[p] = pack_map(*level[p])


def chunk_maps(r, k, v, d, a, x):
    tokens, width = r.shape
    steps = tokens // ROWS
    chunks = tokens // CHUNK
    blk = pl.BlockSpec((ROWS, width), lambda s: (s, 0))
    shapes = [
        pltpu.HBM((tokens, width), BF),
        pltpu.HBM((tokens, width), F32),
        pltpu.HBM((chunks, 2, 128, 128), BF),
        pltpu.HBM((steps, 2, 128, 128), F32),
        pltpu.HBM((steps, 2, 128, 128), F32),
        pltpu.VMEM((2, 128, 128), BF),
    ]
    return pl.pallas_call(
        chunk_kernel,
        grid=(steps,),
        in_specs=[blk] * 6,
        out_specs=[blk, blk] + [whole(s.shape) for s in shapes[2:5]] + [pl.BlockSpec(memory_space=pltpu.VMEM)],
        out_shape=shapes,
        compiler_params=pltpu.CompilerParams(dimension_semantics=("arbitrary",), vmem_limit_bytes=16 << 20),
        name="chunk_maps",
    )(*map(in_hbm, (r, k, v, d, a, x)))


def stage_kernel(count, here_ref, *refs):
    in_m_ref, in_b_ref, pk_ref, g_ref = refs[count:]
    here = here_ref[0]
    for k in range(count):
        g_ref[(here + count - k) % count] = refs[k][...]
    i, j = iotas(128, 128)
    for p in range(2):
        total = unpack_map(g_ref[0, p])
        first = here > 0
        in_m = jnp.where(first, total[0], jnp.where(i == j, 1.0, 0.0))
        in_b = jnp.where(first, total[1], 0.0)
        for k in range(1, count):
            total = compose(total, unpack_map(g_ref[k, p]))
            passed = here > k
            in_m = jnp.where(passed, total[0], in_m)
            in_b = jnp.where(passed, total[1], in_b)
        in_m_ref[p] = in_m
        in_b_ref[p] = in_b
        pk_ref[p] = pack_map(total[0], total[1])


def stage(gathered, here):
    square = pltpu.VMEM((2, 128, 128), F32)
    count = len(gathered)
    vmem = pl.BlockSpec(memory_space=pltpu.VMEM)
    return pl.pallas_call(
        lambda *refs: stage_kernel(count, *refs),
        in_specs=[pl.BlockSpec(memory_space=pltpu.SMEM)] + [vmem] * count,
        out_specs=[vmem] * 3,
        out_shape=[square, square, pltpu.VMEM((2, 128, 128), BF)],
        scratch_shapes=[pltpu.VMEM((count, 2, 128, 128), BF)],
        compiler_params=pltpu.CompilerParams(vmem_limit_bytes=4 << 20),
        name="stage",
    )(here, *map(in_vmem, gathered))


def advance(packed, state):
    i, j = iotas(128, 128)
    packed = packed.astype(F32)
    other = pltpu.roll(packed, 64, 1)
    bd = (i // 64) == (j // 64)
    e = jnp.where(bd, jnp.where(j < 64, packed, other), 0.0).astype(BF)
    b = jnp.where(bd, jnp.where(j < 64, other, packed), 0.0)
    hi, lo = split2(state)
    return state + (mm(e, hi) + mm(e, lo)) + b


def readout_kernel(count, here_ref, *refs):
    my_ref, by_ref, mx_ref, bx_ref, q_ref, o_ref, pc_ref, mg_ref, bg_ref, gate_ref, gain_ref, out_ref, ps_ref, g_ref = refs[count:]
    steps = mg_ref.shape[0]
    tokens = q_ref.shape[0]
    here = here_ref[0]
    for k in range(count):
        g_ref[(here + count - k) % count] = refs[k][...]
    cur = [jnp.zeros((128, 128), F32)] * 2
    for k in range(g_ref.shape[0] - 1):
        for p in range(2):
            m, b = unpack_map(g_ref[k, p])
            cur[p] = jnp.where(here > k, b if k == 0 else mm3(m, cur[p]) + b, cur[p])
    cur = [mm3(my_ref[p], cur[p]) + by_ref[p] for p in range(2)]
    cur = [mm3(mx_ref[p], cur[p]) + bx_ref[p] for p in range(2)]
    for g in range(steps):
        for p in range(2):
            ps_ref[g * GROUP, p] = cur[p]
            if g + 1 < steps:
                cur[p] = mm3(mg_ref[g, p], cur[p]) + bg_ref[g, p]
    for c in range(GROUP - 1):
        for g in range(steps):
            for p in range(2):
                at = g * GROUP + c
                ps_ref[at + 1, p] = advance(pc_ref[at, p], ps_ref[at, p])
    ones = head_ones(256)
    spans = [slice(b, b + ROWS) for b in range(0, tokens, ROWS)]
    outs = []
    for b in range(len(spans)):
        parts = []
        for c in range(b * GROUP, (b + 1) * GROUP):
            rows = slice(c * CHUNK, (c + 1) * CHUNK)
            parts.append(
                jnp.concatenate([mm(q_ref[rows, p * 128 : (p + 1) * 128], ps_ref[c, p].astype(BF)) for p in range(2)], axis=1)
            )
        outs.append(o_ref[spans[b]] + jnp.concatenate(parts, axis=0))
    outs = [o - head_sum(o, ones) * (1.0 / 64) for o in outs]
    sums = [head_sum(o * o, ones) * (1.0 / 64) for o in outs]
    for o, var, rows in zip(outs, sums, spans):
        y = o * lax.rsqrt(var + 0.00064) * gain_ref[...] * gate_ref[rows].astype(F32)
        out_ref[rows] = y.astype(BF)


def readout(gathered, here, maps, q, o, pc, mg, bg, gate, gain):
    tokens, width = q.shape
    count = len(gathered)
    near = (*gathered, *maps)
    far = (q, o, pc, mg, bg, gate, gain.reshape(1, width))
    vmem = pl.BlockSpec(memory_space=pltpu.VMEM)
    return pl.pallas_call(
        lambda *refs: readout_kernel(count, *refs),
        grid=(1,),
        in_specs=[pl.BlockSpec(memory_space=pltpu.SMEM)] + [vmem] * len(near) + [whole(a.shape) for a in far],
        out_specs=vmem,
        out_shape=pltpu.VMEM((tokens, width), BF),
        scratch_shapes=[pltpu.VMEM((tokens // CHUNK, 2, 128, 128), F32), pltpu.VMEM((count, 2, 128, 128), BF)],
        compiler_params=pltpu.CompilerParams(vmem_limit_bytes=16 << 20),
        name="readout",
    )(here, *map(in_vmem, near), *map(in_hbm, far))


def project_kernel(at_ref, *refs):
    m_own, m_right, m_far, m_left, w_near, w_other, w_far, w_far_other, r_right, r_far, r_left, gain_ref = refs[:12]
    w_hbm, r_hbm, normed_ref, stream_ref, w_own, r_own, far_s, normed_s, sems = refs[12:]
    quarter, depth = r_own.shape
    x, core = at_ref[0], at_ref[1]
    w_copy = pltpu.make_async_copy(w_hbm, w_own, sems.at[0])
    r_copy = pltpu.make_async_copy(r_hbm, r_own, sems.at[1])
    w_copy.start()
    r_copy.start()
    half = w_far.shape[0]
    far_s[pl.ds(pl.multiple_of(core * half, half), half)] = w_far[...]
    far_s[pl.ds(pl.multiple_of((1 - core) * half, half), half)] = w_far_other[...]
    w_copy.wait()
    first = core == 0
    writes = []
    for s, rows in ((1, r_right), (2, r_far), (3, r_left), (0, r_own)):
        if s == 0:
            r_copy.wait()
        at = pl.multiple_of((x + s) % 4 * quarter, quarter)
        right, left = m_right[pl.ds(at, quarter)], m_left[pl.ds(at, quarter)]
        part = mm(m_own[pl.ds(at, quarter)], w_own[...]) + mm(m_far[pl.ds(at, quarter)], far_s[...])
        part = part + mm(jnp.where(first, right, left), w_near[...]) + mm(jnp.where(first, left, right), w_other[...])
        stream = (rows[...].astype(F32) + part).astype(BF)
        wide = stream.astype(F32)
        scale = lax.rsqrt(jnp.mean(wide * wide, axis=-1, keepdims=True) + 1e-6)
        normed_s[s] = (wide * scale * gain_ref[...]).astype(BF)
        writes.append(pltpu.make_async_copy(normed_s.at[s], normed_ref.at[pl.ds(at, quarter)], sems.at[2 + s]))
        writes[-1].start()
        if s == 0:
            stream_ref[...] = stream
    for c in writes:
        c.wait()


def project(at, mixed, proj, projs, row, rows, gain):
    tokens, width = mixed[0].shape
    quarter, depth = row.shape
    any_space = pl.BlockSpec(memory_space=pltpu.HBM)
    vmem = pl.BlockSpec(memory_space=pltpu.VMEM)
    near = [*mixed, *projs, *rows, gain.reshape(1, depth)]
    return pl.pallas_call(
        project_kernel,
        grid=(1,),
        in_specs=[pl.BlockSpec(memory_space=pltpu.SMEM)] + [vmem] * len(near) + [any_space] * 2,
        out_specs=[any_space, whole((quarter, depth))],
        out_shape=[pltpu.HBM((tokens, depth), BF), pltpu.HBM((quarter, depth), BF)],
        scratch_shapes=[
            pltpu.VMEM((width, depth), BF),
            pltpu.VMEM((quarter, depth), BF),
            pltpu.VMEM((width, depth), BF),
            pltpu.VMEM((4, quarter, depth), BF),
            pltpu.SemaphoreType.DMA((6,)),
        ],
        compiler_params=pltpu.CompilerParams(vmem_limit_bytes=20 << 20),
        name="project",
    )(at, *map(in_vmem, near), in_hbm(proj), in_hbm(row))


HALO = 16
COLS = 256


def feed_kernel(offsets, load, at_ref, edge_ref, taps_ref, normed_ref, weights_ref, *refs):
    if load:
        out_ref, w_ref, rows_ref, hidden_ref, pre_ref, sems = refs
    else:
        out_ref, rows_ref, hidden_ref, pre_ref, sems = refs
        w_ref = weights_ref
    quarter, depth = out_ref.shape
    width = hidden_ref.shape[1]
    steps = width // COLS
    rest = width - steps * COLS
    starts = [(f * COLS, COLS) for f in range(steps)] + ([(steps * COLS, rest)] if rest else [])
    q = (at_ref[0] + jnp.where(at_ref[1] == 0, offsets[0], offsets[1])) % 4
    before = pl.multiple_of(jnp.maximum(q * quarter - HALO, 0), HALO)
    moves = [
        (normed_ref.at[pl.ds(pl.multiple_of(q * quarter, quarter), quarter)], rows_ref.at[pl.ds(HALO, quarter)]),
        (normed_ref.at[pl.ds(before, HALO)], rows_ref.at[pl.ds(0, HALO)]),
    ]
    if load:
        for at, count in starts:
            for side in range(2):
                part = (slice(None), pl.ds(side * width + at, count))
                moves.append((weights_ref.at[part], w_ref.at[part]))
        for c in range(4):
            part = (pl.ds(c * depth // 4, depth // 4), pl.ds(2 * width, width))
            moves.append((weights_ref.at[part], w_ref.at[part]))
    copies = [pltpu.make_async_copy(a, b, sems.at[i]) for i, (a, b) in enumerate(moves)]
    for c in copies:
        c.start()
    copies[0].wait()
    copies[1].wait()
    rows_ref[:HALO] = jnp.where(q == 0, edge_ref[...], rows_ref[:HALO])

    def product(slot, at, count):
        rows = rows_ref[...]
        for side in range(2):
            cols = pl.ds(pl.multiple_of(side * width + at, 128), count)
            pre_ref[slot, side, :, :count] = mm(rows, w_ref[:, cols]).astype(BF)

    def mixing(slot, at, count):
        mixes = []
        for side in range(2):
            pre = pre_ref[slot, side, :, :count].astype(F32)
            taps = taps_ref[side, :, pl.ds(pl.multiple_of(at, 128), count)]
            mixes.append(taps[0:1] * pltpu.roll(pre, 2, 0) + taps[1:2] * pltpu.roll(pre, 1, 0) + taps[2:3] * pre)
        hid = (mixes[0] / (1.0 + jnp.exp(-mixes[0])) * mixes[1]).astype(BF)
        hidden_ref[:, pl.ds(pl.multiple_of(at, 128), count)] = hid[HALO:]

    def down(at, count):
        cols = pl.ds(pl.multiple_of(at, count), count)
        out_ref[:, cols] = mm_nt(hidden_ref[...], w_ref[cols, 2 * width :]).astype(BF)

    part = depth // 4
    if load:
        for f, (at, count) in enumerate(starts):
            copies[2 + 2 * f].wait()
            copies[3 + 2 * f].wait()
            product(f % 2, at, count)
            if f:
                mixing((f - 1) % 2, *starts[f - 1])
        mixing((len(starts) - 1) % 2, *starts[-1])
        for h in range(4):
            copies[2 + 2 * len(starts) + h].wait()
            down(h * part, part)
        return
    product(0, 0, COLS)

    def turn(f, carry):
        product(f % 2, f * COLS, COLS)
        mixing((f - 1) % 2, (f - 1) * COLS, COLS)
        return carry

    lax.fori_loop(1, steps, turn, 0)
    if rest:
        product(steps % 2, *starts[-1])
    mixing((steps - 1) % 2, (steps - 1) * COLS, COLS)
    if rest:
        mixing(steps % 2, *starts[-1])

    def down_turn(h, carry):
        down(h * part, part)
        return carry

    lax.fori_loop(0, 4, down_turn, 0)


def feed(offsets, load, at, normed, edge, weights, taps):
    tokens, depth = normed.shape
    quarter = tokens // 4
    width = weights.shape[1] // 3
    vmem = pl.BlockSpec(memory_space=pltpu.VMEM)
    hbm = pl.BlockSpec(memory_space=pltpu.HBM)
    out = jax.ShapeDtypeStruct((quarter, depth), BF)
    return pl.pallas_call(
        lambda *refs: feed_kernel(offsets, load, *refs),
        in_specs=[pl.BlockSpec(memory_space=pltpu.SMEM), vmem, vmem, hbm, hbm if load else vmem],
        out_specs=[vmem, vmem] if load else vmem,
        scratch_shapes=[
            pltpu.VMEM((quarter + HALO, depth), BF),
            pltpu.VMEM((quarter, width), BF),
            pltpu.VMEM((2, 2, quarter + HALO, COLS), BF),
            pltpu.SemaphoreType.DMA((24 if load else 2,)),
        ],
        out_shape=[out, pltpu.VMEM(weights.shape, BF)] if load else out,
        compiler_params=pltpu.CompilerParams(vmem_limit_bytes=10 << 20),
        name="feed",
    )(at, edge, taps, in_hbm(normed), in_hbm(weights) if load else in_vmem(weights))


def shifted(x, by):
    n = lax.axis_size("tp")
    return lax.ppermute(x, "tp", [(i, (i + by) % n) for i in range(n)])


def by_core(x, first, second):
    n = lax.axis_size("tp")
    pairs = [(i, (i + first) % n) for i in range(n)] + [(n + i, n + (i + second) % n) for i in range(n)]
    return lax.ppermute(x, ("sp_2", "tp"), pairs)


def swapped(x):
    return lax.ppermute(x, "sp_2", [(0, 1), (1, 0)])


def passed_along(x, axis, by):
    count = lax.axis_size(axis)
    pairs = [(i, i + by) for i in range(count) if 0 <= i + by < count]
    return lax.ppermute(x, axis, pairs)


def everyone(x, axis):
    n = lax.axis_size(axis)
    return [x] + [lax.ppermute(x, axis, [(i, (i + by) % n) for i in range(n)]) for by in range(1, n)]


def body(
    residual_input_stream,
    receptance,
    key_matrix_all,
    value_matrix_all,
    decay_preactivation,
    learning_rate_preactivation,
    output_gate_all_heads,
    extra_log_decay,
    head_norm_gain,
    output_projection_weight,
    feedforward_norm_gain,
    gate_projection_weight,
    up_projection_weight,
    down_projection_weight,
    convolution_kernel,
):
    x = lax.axis_index("tp").astype(jnp.int32)
    core = lax.axis_index("sp_2").astype(jnp.int32)
    first = core == 0
    at = jnp.stack([x, core])
    places = [lax.axis_index(axis).astype(jnp.int32).reshape(1) for axis in SP]
    receptance, at, first, places = lax.optimization_barrier((receptance, at, first, places))
    local = jnp.concatenate([gate_projection_weight, up_projection_weight, down_projection_weight], axis=1)
    weights = lax.all_gather(local, SP, axis=0, tiled=True)
    taps = convolution_kernel.astype(F32).transpose(1, 0, 2)

    row_left, row_right = shifted(residual_input_stream, 1), shifted(residual_input_stream, -1)
    proj_near = by_core(output_projection_weight, -1, 1)

    q, o, pc, mg, bg, pk = chunk_maps(
        receptance,
        key_matrix_all,
        value_matrix_all,
        decay_preactivation,
        learning_rate_preactivation,
        extra_log_decay,
    )
    mx, bx, pk = stage(everyone(pk, "sp_2"), places[2])
    my, by, pk = stage(everyone(pk, "sp_1"), places[1])
    by, row_left, row_right, proj_near = lax.optimization_barrier((by, row_left, row_right, proj_near))
    half = proj_near.shape[0] // 2
    row_far = by_core(jnp.where(first, row_left, row_right), 1, -1)
    proj_far = by_core(jnp.where(first, proj_near[:half], proj_near[half:]), -1, 1)
    proj_other = swapped(proj_near)
    mixed = readout(
        everyone(pk, "sp_0"), places[0], (my, by, mx, bx), q, o, pc, mg, bg, output_gate_all_heads, head_norm_gain
    )
    mixed, row_far, proj_far, proj_other = lax.optimization_barrier((mixed, row_far, proj_far, proj_other))
    mixed_left, mixed_right = shifted(mixed, 1), shifted(mixed, -1)
    proj_far_other = swapped(proj_far)
    mixed_far = by_core(jnp.where(first, mixed_left, mixed_right), 1, -1)
    normed, stream = project(
        at,
        (mixed, mixed_right, mixed_far, mixed_left),
        output_projection_weight,
        (proj_near, proj_other, proj_far, proj_far_other),
        residual_input_stream,
        (row_right, row_far, row_left),
        feedforward_norm_gain,
    )
    edge = passed_along(normed[-HALO:], SP, 1)
    wide = lambda t: t.astype(F32)
    far, weights = feed((2, 2), True, at, normed, edge, weights, taps)
    far = by_core(far, 1, -1)
    early = by_core(feed((3, 1), False, at, normed, edge, weights, taps), -1, 1)
    late = feed((1, 3), False, at, normed, edge, weights, taps)
    late = by_core((wide(late) + wide(far)).astype(BF), 1, -1)
    own = feed((0, 0), False, at, normed, edge, weights, taps)
    return (wide(stream) + (wide(own) + wide(early) + wide(late))).astype(BF)


def solution(mesh):
    split = Mesh(mesh.devices.reshape(4, 4, 2, mesh.shape["tp"]), ("sp_0", "sp_1", "sp_2", "tp"))
    in_specs = (
        P(SP_TP, None),
        P(SP, "tp"),
        P(SP, "tp"),
        P(SP, "tp"),
        P(SP, "tp"),
        P(SP, "tp"),
        P(SP, "tp"),
        P(SP, "tp"),
        P("tp"),
        P("tp", None),
        P(),
        P(SP, "tp"),
        P(SP, "tp"),
        P(SP, "tp"),
        P(None, None, "tp"),
    )
    out_specs = P(SP_TP, None)
    return jax.shard_map(body, mesh=split, in_specs=in_specs, out_specs=out_specs, check_vma=False)
```

```python
import jax
import jax.numpy as jnp
from jax import lax
from jax.experimental import pallas as pl
from jax.experimental.pallas import tpu as pltpu
from jax.sharding import Mesh
from jax.sharding import PartitionSpec as P


SP = ("sp_0", "sp_1", "sp_2")
SP_TP = ("sp_0", "sp_1", "sp_2", "tp")

BF = jnp.bfloat16
F32 = jnp.float32
CHUNK = 64
GROUP = 4
ROWS = CHUNK * GROUP


def in_hbm(x):
    return pltpu.with_memory_space_constraint(x, pltpu.HBM)


def in_vmem(x):
    return pltpu.with_memory_space_constraint(x, pltpu.VMEM)


def whole(shape):
    return pl.BlockSpec(tuple(shape), lambda *_: (0,) * len(shape))


def mm(a, b):
    return lax.dot_general(a, b, (((1,), (0,)), ((), ())), preferred_element_type=F32)


def mm_nt(a, b):
    return lax.dot_general(a, b, (((1,), (1,)), ((), ())), preferred_element_type=F32)


def split2(x):
    hi = x.astype(BF)
    return hi, (x - hi.astype(F32)).astype(BF)


def mm3(a, b):
    ah, al = split2(a)
    bh, bl = split2(b)
    return mm(ah, bh) + (mm(ah, bl) + mm(al, bh))


def iotas(n, m):
    return lax.broadcasted_iota(jnp.int32, (n, m), 0), lax.broadcasted_iota(jnp.int32, (n, m), 1)


def head_ones(n):
    i, j = iotas(n, n)
    return jnp.where((i // 64) == (j // 64), 1.0, 0.0).astype(BF)


def head_sum(x, ones):
    hi, lo = split2(x)
    return mm(hi, ones) + mm(lo, ones)


def pack_map(m, b):
    i, j = iotas(128, 128)
    e = m - jnp.where(i == j, 1.0, 0.0)
    return jnp.where(j < 64, e + pltpu.roll(e, 64, 1), b + pltpu.roll(b, 64, 1)).astype(BF)


def unpack_map(p):
    i, j = iotas(128, 128)
    p = p.astype(F32)
    s = pltpu.roll(p, 64, 1)
    bd = (i // 64) == (j // 64)
    m = jnp.where(bd, jnp.where(j < 64, p, s), 0.0) + jnp.where(i == j, 1.0, 0.0)
    b = jnp.where(bd, jnp.where(j < 64, s, p), 0.0)
    return m, b


def compose(first, second):
    both = mm3(second[0], jnp.concatenate([first[0], first[1]], axis=1))
    return both[:, :128], both[:, 128:] + second[1]


def tree(level):
    while len(level) > 1:
        level = [[compose(level[z][p], level[z + 1][p]) for p in range(2)] for z in range(0, len(level), 2)]
    return level[0]


def chunk_kernel(r_ref, k_ref, v_ref, d_ref, a_ref, x_ref, q_ref, o_ref, pc_ref, mg_ref, bg_ref, pk_ref):
    step = pl.program_id(0)
    ones = head_ones(256)
    k = k_ref[...].astype(F32)
    n = k * lax.rsqrt(head_sum(k * k, ones) + 1e-6)
    rate = 1.0 / (1.0 + jnp.exp(-a_ref[...].astype(F32)))
    b = n * rate
    ld = (-0.6065306597126334) / (1.0 + jnp.exp(-d_ref[...].astype(F32))) + x_ref[...]
    i, j = iotas(ROWS, ROWS)
    tri = jnp.where(((i // CHUNK) == (j // CHUNK)) & (i >= j), 1.0, 0.0).astype(BF)
    ldh, ldl = split2(ld)
    g = mm(tri, ldh) + mm(tri, ldl)
    mids = [g[c * CHUNK + CHUNK // 2 : c * CHUNK + CHUNK // 2 + 1] for c in range(GROUP)]
    ends = [g[c * CHUNK + CHUNK - 1 : c * CHUNK + CHUNK] for c in range(GROUP)]
    rel = jnp.concatenate([g[c * CHUNK : (c + 1) * CHUNK] - mids[c] for c in range(GROUP)], axis=0)
    up = jnp.exp(rel)
    prev = jnp.exp(rel - ld)
    down = jnp.exp(-rel)
    rq = r_ref[...].astype(F32) * up
    nq = n * prev
    kk = k * down
    bb = b * down
    v = v_ref[...]

    i, j = iotas(128, 128)
    bd = (i // 64) == (j // 64)
    ti, tj = i % 64, j % 64
    strict = bd & (ti > tj)
    within = bd & (ti >= tj)
    eye = jnp.where(i == j, 1.0, 0.0)
    mask_a = jnp.concatenate([jnp.concatenate([strict, strict], axis=1), jnp.concatenate([within, within], axis=1)], axis=0)
    low = lax.broadcasted_iota(jnp.int32, (64, 128), 1) < 64
    zero = jnp.zeros((64, 128), BF)

    def spread(x):
        return jnp.concatenate([jnp.where(low, x, zero), jnp.where(low, zero, x)], axis=0)

    def fold(x):
        return jnp.where(low, x[:64], x[64:])

    units = [(c, p) for c in range(GROUP) for p in range(2)]

    def cut(x, u):
        c, p = u
        return x[c * CHUNK : (c + 1) * CHUNK, p * 128 : (p + 1) * 128]

    st = {}
    for u in units:
        nqb = spread(cut(nq, u).astype(BF))
        rqb = spread(cut(rq, u).astype(BF))
        kb = cut(kk, u).astype(BF)
        bbb = cut(bb, u).astype(BF)
        vb = cut(v, u)
        att = mm_nt(jnp.concatenate([nqb, rqb], axis=0), jnp.concatenate([kb, kb, bbb, bbb], axis=0))
        st[u] = dict(nqb=nqb, rqb=rqb, vb=vb, att=att)
    for u in units:
        t = st[u]
        att = t.pop("att")
        t["L"] = jnp.where(strict, att[:128, 128:], 0.0)
        t["arb"] = jnp.where(within, att[128:, 128:], 0.0).astype(BF)
        t["ak"] = jnp.concatenate(
            [jnp.where(strict, att[:128, :128], 0.0).astype(BF), jnp.where(within, att[128:, :128], 0.0).astype(BF)], axis=0
        )
    lev = jnp.where(bd & ((ti // 2) == (tj // 2)), 1.0, 0.0)
    for u in units:
        st[u]["X"] = eye - st[u]["L"] * lev
    s = 2
    while s < CHUNK:
        lev = ((i // (2 * s)) == (j // (2 * s))) & ((i // s) > (j // s))
        for u in units:
            x = st[u]["X"]
            xb = x.astype(BF)
            c = jnp.where(lev, st[u]["L"], 0.0).astype(BF)
            y = mm(xb, c).astype(BF)
            st[u]["X"] = x - mm(y, xb)
        s *= 2
    for u in units:
        t = st[u]
        kv = mm(t["ak"], spread(t["vb"]))
        t["av"], t["ov"] = kv[:128].astype(BF), kv[128:]
    for u in units:
        t = st[u]
        t["wu"] = mm(t["X"].astype(BF), jnp.concatenate([t["nqb"], t["av"]], axis=1))
    for u in units:
        t = st[u]
        t["f"] = mm(t["arb"], t["wu"].astype(BF))
    for u in units:
        t = st[u]
        c, p = u
        wu = t["wu"]
        tail = jnp.exp(ends[c][:, p * 128 : (p + 1) * 128] - mids[c][:, p * 128 : (p + 1) * 128])
        left = jnp.concatenate([cut(kk, u) * tail, cut(bb, u) * tail], axis=0).T.astype(BF)
        right = jnp.concatenate(
            [
                jnp.concatenate([t["vb"], zero], axis=1),
                jnp.concatenate([-fold(wu[:, 128:]), fold(wu[:, :128])], axis=1).astype(BF),
            ],
            axis=0,
        )
        t["be"] = mm(left, right)
    maps = {}
    for u in units:
        t = st[u]
        c, p = u
        f = t["f"]
        lanes = slice(p * 128, (p + 1) * 128)
        emid = jnp.exp(mids[c][:, lanes])
        q = fold(t["rqb"].astype(F32) - f[:, :128]) * emid
        rows = slice(c * CHUNK, (c + 1) * CHUNK)
        q_ref[rows, lanes] = q.astype(BF)
        o_ref[rows, lanes] = fold(t["ov"] - f[:, 128:])
        be = t["be"]
        m = jnp.where(i == j, jnp.exp(ends[c][:, lanes]), 0.0) - jnp.where(bd, be[:, 128:], 0.0) * emid
        bm = jnp.where(bd, be[:, :128], 0.0)
        maps[u] = (m, bm)
        pc_ref[step * GROUP + c, p] = pack_map(m, bm)
    level = [[maps[(c, p)] for p in range(2)] for c in range(GROUP)]
    level = tree(level)
    for p in range(2):
        mg_ref[step, p], bg_ref[step, p] = level[p]

    @pl.when(step == pl.num_programs(0) - 1)
    def _():
        level = tree([[(mg_ref[z, p], bg_ref[z, p]) for p in range(2)] for z in range(mg_ref.shape[0])])
        for p in range(2):
            pk_ref[p] = pack_map(*level[p])


def chunk_maps(r, k, v, d, a, x):
    tokens, width = r.shape
    steps = tokens // ROWS
    chunks = tokens // CHUNK
    blk = pl.BlockSpec((ROWS, width), lambda s: (s, 0))
    shapes = [
        pltpu.HBM((tokens, width), BF),
        pltpu.HBM((tokens, width), F32),
        pltpu.HBM((chunks, 2, 128, 128), BF),
        pltpu.HBM((steps, 2, 128, 128), F32),
        pltpu.HBM((steps, 2, 128, 128), F32),
        pltpu.VMEM((2, 128, 128), BF),
    ]
    return pl.pallas_call(
        chunk_kernel,
        grid=(steps,),
        in_specs=[blk] * 6,
        out_specs=[blk, blk] + [whole(s.shape) for s in shapes[2:5]] + [pl.BlockSpec(memory_space=pltpu.VMEM)],
        out_shape=shapes,
        compiler_params=pltpu.CompilerParams(dimension_semantics=("arbitrary",), vmem_limit_bytes=16 << 20),
        name="chunk_maps",
    )(*map(in_hbm, (r, k, v, d, a, x)))


def stage_kernel(count, here_ref, *refs):
    in_m_ref, in_b_ref, pk_ref, g_ref = refs[count:]
    here = here_ref[0]
    for k in range(count):
        g_ref[(here + count - k) % count] = refs[k][...]
    i, j = iotas(128, 128)
    for p in range(2):
        total = unpack_map(g_ref[0, p])
        first = here > 0
        in_m = jnp.where(first, total[0], jnp.where(i == j, 1.0, 0.0))
        in_b = jnp.where(first, total[1], 0.0)
        for k in range(1, count):
            total = compose(total, unpack_map(g_ref[k, p]))
            passed = here > k
            in_m = jnp.where(passed, total[0], in_m)
            in_b = jnp.where(passed, total[1], in_b)
        in_m_ref[p] = in_m
        in_b_ref[p] = in_b
        pk_ref[p] = pack_map(total[0], total[1])


def stage(gathered, here):
    square = pltpu.VMEM((2, 128, 128), F32)
    count = len(gathered)
    vmem = pl.BlockSpec(memory_space=pltpu.VMEM)
    return pl.pallas_call(
        lambda *refs: stage_kernel(count, *refs),
        in_specs=[pl.BlockSpec(memory_space=pltpu.SMEM)] + [vmem] * count,
        out_specs=[vmem] * 3,
        out_shape=[square, square, pltpu.VMEM((2, 128, 128), BF)],
        scratch_shapes=[pltpu.VMEM((count, 2, 128, 128), BF)],
        compiler_params=pltpu.CompilerParams(vmem_limit_bytes=4 << 20),
        name="stage",
    )(here, *map(in_vmem, gathered))


def advance(packed, state):
    i, j = iotas(128, 128)
    packed = packed.astype(F32)
    other = pltpu.roll(packed, 64, 1)
    bd = (i // 64) == (j // 64)
    e = jnp.where(bd, jnp.where(j < 64, packed, other), 0.0).astype(BF)
    b = jnp.where(bd, jnp.where(j < 64, other, packed), 0.0)
    hi, lo = split2(state)
    return state + (mm(e, hi) + mm(e, lo)) + b


def readout_kernel(count, here_ref, *refs):
    my_ref, by_ref, mx_ref, bx_ref, q_ref, o_ref, pc_ref, mg_ref, bg_ref, gate_ref, gain_ref, out_ref, ps_ref, g_ref = refs[count:]
    steps = mg_ref.shape[0]
    tokens = q_ref.shape[0]
    here = here_ref[0]
    for k in range(count):
        g_ref[(here + count - k) % count] = refs[k][...]
    cur = [jnp.zeros((128, 128), F32)] * 2
    for k in range(g_ref.shape[0] - 1):
        for p in range(2):
            m, b = unpack_map(g_ref[k, p])
            cur[p] = jnp.where(here > k, b if k == 0 else mm3(m, cur[p]) + b, cur[p])
    cur = [mm3(my_ref[p], cur[p]) + by_ref[p] for p in range(2)]
    cur = [mm3(mx_ref[p], cur[p]) + bx_ref[p] for p in range(2)]
    for g in range(steps):
        for p in range(2):
            ps_ref[g * GROUP, p] = cur[p]
            if g + 1 < steps:
                cur[p] = mm3(mg_ref[g, p], cur[p]) + bg_ref[g, p]
    for c in range(GROUP - 1):
        for g in range(steps):
            for p in range(2):
                at = g * GROUP + c
                ps_ref[at + 1, p] = advance(pc_ref[at, p], ps_ref[at, p])
    ones = head_ones(256)
    spans = [slice(b, b + ROWS) for b in range(0, tokens, ROWS)]
    outs = []
    for b in range(len(spans)):
        parts = []
        for c in range(b * GROUP, (b + 1) * GROUP):
            rows = slice(c * CHUNK, (c + 1) * CHUNK)
            parts.append(
                jnp.concatenate([mm(q_ref[rows, p * 128 : (p + 1) * 128], ps_ref[c, p].astype(BF)) for p in range(2)], axis=1)
            )
        outs.append(o_ref[spans[b]] + jnp.concatenate(parts, axis=0))
    outs = [o - head_sum(o, ones) * (1.0 / 64) for o in outs]
    sums = [head_sum(o * o, ones) * (1.0 / 64) for o in outs]
    for o, var, rows in zip(outs, sums, spans):
        y = o * lax.rsqrt(var + 0.00064) * gain_ref[...] * gate_ref[rows].astype(F32)
        out_ref[rows] = y.astype(BF)


def readout(gathered, here, maps, q, o, pc, mg, bg, gate, gain):
    tokens, width = q.shape
    count = len(gathered)
    near = (*gathered, *maps)
    far = (q, o, pc, mg, bg, gate, gain.reshape(1, width))
    vmem = pl.BlockSpec(memory_space=pltpu.VMEM)
    return pl.pallas_call(
        lambda *refs: readout_kernel(count, *refs),
        grid=(1,),
        in_specs=[pl.BlockSpec(memory_space=pltpu.SMEM)] + [vmem] * len(near) + [whole(a.shape) for a in far],
        out_specs=vmem,
        out_shape=pltpu.VMEM((tokens, width), BF),
        scratch_shapes=[pltpu.VMEM((tokens // CHUNK, 2, 128, 128), F32), pltpu.VMEM((count, 2, 128, 128), BF)],
        compiler_params=pltpu.CompilerParams(vmem_limit_bytes=16 << 20),
        name="readout",
    )(here, *map(in_vmem, near), *map(in_hbm, far))


def partial_kernel(at_ref, m_own, m_right, m_left, w_own, w_near, w_other, r_own, r_right, r_far, r_left, acc_ref):
    quarter = r_own.shape[0]
    first = at_ref[1] == 0
    for s, rows in enumerate((r_own, r_right, r_far, r_left)):
        at = pl.multiple_of((at_ref[0] + s) % 4 * quarter, quarter)
        right, left = m_right[pl.ds(at, quarter)], m_left[pl.ds(at, quarter)]
        part = mm(m_own[pl.ds(at, quarter)], w_own[...]) + mm(jnp.where(first, right, left), w_near[...])
        acc_ref[s] = rows[...].astype(F32) + (part + mm(jnp.where(first, left, right), w_other[...]))


def project_kernel(at_ref, acc_ref, m_far, w_far, w_far_other, gain_ref, normed_ref, stream_ref, edge_ref, far_s, normed_s, sems):
    _, quarter, _ = acc_ref.shape
    x, core = at_ref[0], at_ref[1]
    half = w_far.shape[0]
    far_s[pl.ds(pl.multiple_of(core * half, half), half)] = w_far[...]
    far_s[pl.ds(pl.multiple_of((1 - core) * half, half), half)] = w_far_other[...]
    writes = []
    for s in range(4):
        q = (x + s) % 4
        at = pl.multiple_of(q * quarter, quarter)
        stream = (acc_ref[s] + mm(m_far[pl.ds(at, quarter)], far_s[...])).astype(BF)
        wide = stream.astype(F32)
        scale = lax.rsqrt(jnp.mean(wide * wide, axis=-1, keepdims=True) + 1e-6)
        normed = (wide * scale * gain_ref[...]).astype(BF)
        normed_s[s] = normed
        writes.append(pltpu.make_async_copy(normed_s.at[s], normed_ref.at[pl.ds(at, quarter)], sems.at[s]))
        writes[-1].start()
        if s == 0:
            stream_ref[...] = stream

        @pl.when(q == 3)
        def _(s=s):
            edge_ref[...] = normed_s[s, quarter - HALO :]

    for c in writes:
        c.wait()


def project_partial(at, mixed, projs, rows):
    quarter, depth = rows[0].shape
    vmem = pl.BlockSpec(memory_space=pltpu.VMEM)
    near = [*mixed, *projs, *rows]
    return pl.pallas_call(
        partial_kernel,
        in_specs=[pl.BlockSpec(memory_space=pltpu.SMEM)] + [vmem] * len(near),
        out_specs=vmem,
        out_shape=pltpu.VMEM((4, quarter, depth), F32),
        compiler_params=pltpu.CompilerParams(vmem_limit_bytes=10 << 20),
        name="project_partial",
    )(at, *map(in_vmem, near))


def project(at, acc, m_far, w_far, w_far_other, gain):
    tokens, width = m_far.shape
    _, quarter, depth = acc.shape
    vmem = pl.BlockSpec(memory_space=pltpu.VMEM)
    near = [acc, m_far, w_far, w_far_other, gain.reshape(1, depth)]
    return pl.pallas_call(
        project_kernel,
        grid=(1,),
        in_specs=[pl.BlockSpec(memory_space=pltpu.SMEM)] + [vmem] * len(near),
        out_specs=[pl.BlockSpec(memory_space=pltpu.HBM), whole((quarter, depth)), vmem],
        out_shape=[pltpu.HBM((tokens, depth), BF), pltpu.HBM((quarter, depth), BF), pltpu.VMEM((HALO, depth), BF)],
        scratch_shapes=[
            pltpu.VMEM((width, depth), BF),
            pltpu.VMEM((4, quarter, depth), BF),
            pltpu.SemaphoreType.DMA((4,)),
        ],
        compiler_params=pltpu.CompilerParams(vmem_limit_bytes=16 << 20),
        name="project",
    )(at, *map(in_vmem, near))


HALO = 16
COLS = 256


def feed_kernel(offsets, load, at_ref, edge_ref, taps_ref, normed_ref, weights_ref, *refs):
    if load:
        out_ref, w_ref, rows_ref, hidden_ref, pre_ref, sems = refs
    else:
        out_ref, rows_ref, hidden_ref, pre_ref, sems = refs
        w_ref = weights_ref
    quarter, depth = out_ref.shape
    width = hidden_ref.shape[1]
    steps = width // COLS
    rest = width - steps * COLS
    starts = [(f * COLS, COLS) for f in range(steps)] + ([(steps * COLS, rest)] if rest else [])
    q = (at_ref[0] + jnp.where(at_ref[1] == 0, offsets[0], offsets[1])) % 4
    before = pl.multiple_of(jnp.maximum(q * quarter - HALO, 0), HALO)
    moves = [
        (normed_ref.at[pl.ds(pl.multiple_of(q * quarter, quarter), quarter)], rows_ref.at[pl.ds(HALO, quarter)]),
        (normed_ref.at[pl.ds(before, HALO)], rows_ref.at[pl.ds(0, HALO)]),
    ]
    if load:
        for at, count in starts:
            for side in range(2):
                part = (slice(None), pl.ds(side * width + at, count))
                moves.append((weights_ref.at[part], w_ref.at[part]))
        for c in range(4):
            part = (pl.ds(c * depth // 4, depth // 4), pl.ds(2 * width, width))
            moves.append((weights_ref.at[part], w_ref.at[part]))
    copies = [pltpu.make_async_copy(a, b, sems.at[i]) for i, (a, b) in enumerate(moves)]
    for c in copies:
        c.start()
    copies[0].wait()
    copies[1].wait()
    rows_ref[:HALO] = jnp.where(q == 0, edge_ref[...], rows_ref[:HALO])

    def product(slot, at, count):
        rows = rows_ref[...]
        for side in range(2):
            cols = pl.ds(pl.multiple_of(side * width + at, 128), count)
            pre_ref[slot, side, :, :count] = mm(rows, w_ref[:, cols]).astype(BF)

    def mixing(slot, at, count):
        mixes = []
        for side in range(2):
            pre = pre_ref[slot, side, :, :count].astype(F32)
            taps = taps_ref[side, :, pl.ds(pl.multiple_of(at, 128), count)]
            mixes.append(taps[0:1] * pltpu.roll(pre, 2, 0) + taps[1:2] * pltpu.roll(pre, 1, 0) + taps[2:3] * pre)
        hid = (mixes[0] / (1.0 + jnp.exp(-mixes[0])) * mixes[1]).astype(BF)
        hidden_ref[:, pl.ds(pl.multiple_of(at, 128), count)] = hid[HALO:]

    def down(at, count):
        cols = pl.ds(pl.multiple_of(at, count), count)
        out_ref[:, cols] = mm_nt(hidden_ref[...], w_ref[cols, 2 * width :]).astype(BF)

    part = depth // 4
    if load:
        for f, (at, count) in enumerate(starts):
            copies[2 + 2 * f].wait()
            copies[3 + 2 * f].wait()
            product(f % 2, at, count)
            if f:
                mixing((f - 1) % 2, *starts[f - 1])
        mixing((len(starts) - 1) % 2, *starts[-1])
        for h in range(4):
            copies[2 + 2 * len(starts) + h].wait()
            down(h * part, part)
        return
    product(0, 0, COLS)

    def turn(f, carry):
        product(f % 2, f * COLS, COLS)
        mixing((f - 1) % 2, (f - 1) * COLS, COLS)
        return carry

    lax.fori_loop(1, steps, turn, 0)
    if rest:
        product(steps % 2, *starts[-1])
    mixing((steps - 1) % 2, (steps - 1) * COLS, COLS)
    if rest:
        mixing(steps % 2, *starts[-1])

    def down_turn(h, carry):
        down(h * part, part)
        return carry

    lax.fori_loop(0, 4, down_turn, 0)


def feed(offsets, load, at, normed, edge, weights, taps):
    tokens, depth = normed.shape
    quarter = tokens // 4
    width = weights.shape[1] // 3
    vmem = pl.BlockSpec(memory_space=pltpu.VMEM)
    hbm = pl.BlockSpec(memory_space=pltpu.HBM)
    out = jax.ShapeDtypeStruct((quarter, depth), BF)
    return pl.pallas_call(
        lambda *refs: feed_kernel(offsets, load, *refs),
        in_specs=[pl.BlockSpec(memory_space=pltpu.SMEM), vmem, vmem, hbm, hbm if load else vmem],
        out_specs=[vmem, vmem] if load else vmem,
        scratch_shapes=[
            pltpu.VMEM((quarter + HALO, depth), BF),
            pltpu.VMEM((quarter, width), BF),
            pltpu.VMEM((2, 2, quarter + HALO, COLS), BF),
            pltpu.SemaphoreType.DMA((24 if load else 2,)),
        ],
        out_shape=[out, pltpu.VMEM(weights.shape, BF)] if load else out,
        compiler_params=pltpu.CompilerParams(vmem_limit_bytes=10 << 20),
        name="feed",
    )(at, edge, taps, in_hbm(normed), in_hbm(weights) if load else in_vmem(weights))


def shifted(x, by):
    n = lax.axis_size("tp")
    return lax.ppermute(x, "tp", [(i, (i + by) % n) for i in range(n)])


def by_core(x, first, second):
    n = lax.axis_size("tp")
    pairs = [(i, (i + first) % n) for i in range(n)] + [(n + i, n + (i + second) % n) for i in range(n)]
    return lax.ppermute(x, ("sp_2", "tp"), pairs)


def swapped(x):
    return lax.ppermute(x, "sp_2", [(0, 1), (1, 0)])


def passed_along(x, axis, by):
    count = lax.axis_size(axis)
    pairs = [(i, i + by) for i in range(count) if 0 <= i + by < count]
    return lax.ppermute(x, axis, pairs)


def everyone(x, axis):
    n = lax.axis_size(axis)
    return [x] + [lax.ppermute(x, axis, [(i, (i + by) % n) for i in range(n)]) for by in range(1, n)]


def body(
    residual_input_stream,
    receptance,
    key_matrix_all,
    value_matrix_all,
    decay_preactivation,
    learning_rate_preactivation,
    output_gate_all_heads,
    extra_log_decay,
    head_norm_gain,
    output_projection_weight,
    feedforward_norm_gain,
    gate_projection_weight,
    up_projection_weight,
    down_projection_weight,
    convolution_kernel,
):
    x = lax.axis_index("tp").astype(jnp.int32)
    core = lax.axis_index("sp_2").astype(jnp.int32)
    first = core == 0
    at = jnp.stack([x, core])
    places = [lax.axis_index(axis).astype(jnp.int32).reshape(1) for axis in SP]
    receptance, at, first, places = lax.optimization_barrier((receptance, at, first, places))
    local = jnp.concatenate([gate_projection_weight, up_projection_weight, down_projection_weight], axis=1)
    weights = lax.all_gather(local, SP, axis=0, tiled=True)
    taps = convolution_kernel.astype(F32).transpose(1, 0, 2)

    row_left, row_right = shifted(residual_input_stream, 1), shifted(residual_input_stream, -1)
    proj_near = by_core(output_projection_weight, -1, 1)

    q, o, pc, mg, bg, pk = chunk_maps(
        receptance,
        key_matrix_all,
        value_matrix_all,
        decay_preactivation,
        learning_rate_preactivation,
        extra_log_decay,
    )
    mx, bx, pk = stage(everyone(pk, "sp_2"), places[2])
    pieces = everyone(pk, "sp_1")
    my, by, pk = stage(pieces, places[1])
    half = proj_near.shape[0] // 2
    row_far = by_core(jnp.where(first, row_left, row_right), 1, -1)
    proj_far = by_core(jnp.where(first, proj_near[:half], proj_near[half:]), -1, 1)
    proj_other = swapped(proj_near)
    pieces = everyone(pk, "sp_0")
    mixed = readout(
        pieces, places[0], (my, by, mx, bx), q, o, pc, mg, bg, output_gate_all_heads, head_norm_gain
    )
    mixed_left, mixed_right = shifted(mixed, 1), shifted(mixed, -1)
    proj_far_other = swapped(proj_far)
    mixed_far = by_core(jnp.where(first, mixed_left, mixed_right), 1, -1)
    acc = project_partial(
        at,
        (mixed, mixed_right, mixed_left),
        (output_projection_weight, proj_near, proj_other),
        (residual_input_stream, row_right, row_far, row_left),
    )
    normed, stream, edge = project(at, acc, mixed_far, proj_far, proj_far_other, feedforward_norm_gain)
    edge = passed_along(edge, SP, 1)
    wide = lambda t: t.astype(F32)
    far, weights = feed((2, 2), True, at, normed, edge, weights, taps)
    far = by_core(far, 1, -1)
    early = by_core(feed((3, 1), False, at, normed, edge, weights, taps), -1, 1)
    late = feed((1, 3), False, at, normed, edge, weights, taps)
    late = by_core((wide(late) + wide(far)).astype(BF), 1, -1)
    own = feed((0, 0), False, at, normed, edge, weights, taps)
    return (wide(stream) + (wide(own) + wide(early) + wide(late))).astype(BF)


def solution(mesh):
    split = Mesh(mesh.devices.reshape(4, 4, 2, mesh.shape["tp"]), ("sp_0", "sp_1", "sp_2", "tp"))
    in_specs = (
        P(SP_TP, None),
        P(SP, "tp"),
        P(SP, "tp"),
        P(SP, "tp"),
        P(SP, "tp"),
        P(SP, "tp"),
        P(SP, "tp"),
        P(SP, "tp"),
        P("tp"),
        P("tp", None),
        P(),
        P(SP, "tp"),
        P(SP, "tp"),
        P(SP, "tp"),
        P(None, None, "tp"),
    )
    out_specs = P(SP_TP, None)

    return jax.shard_map(body, mesh=split, in_specs=in_specs, out_specs=out_specs, check_vma=False)
```

```python
import jax
import jax.numpy as jnp
from jax import lax
from jax.experimental import pallas as pl
from jax.experimental.pallas import tpu as pltpu
from jax.sharding import Mesh
from jax.sharding import PartitionSpec as P


SP = ("sp_0", "sp_1", "sp_2")
SP_TP = ("sp_0", "sp_1", "sp_2", "tp")

BF = jnp.bfloat16
F32 = jnp.float32
CHUNK = 64
GROUP = 4
ROWS = CHUNK * GROUP


def in_hbm(x):
    return pltpu.with_memory_space_constraint(x, pltpu.HBM)


def in_vmem(x):
    return pltpu.with_memory_space_constraint(x, pltpu.VMEM)


def whole(shape):
    return pl.BlockSpec(tuple(shape), lambda *_: (0,) * len(shape))


def mm(a, b):
    return lax.dot_general(a, b, (((1,), (0,)), ((), ())), preferred_element_type=F32)


def mm_nt(a, b):
    return lax.dot_general(a, b, (((1,), (1,)), ((), ())), preferred_element_type=F32)


def split2(x):
    hi = x.astype(BF)
    return hi, (x - hi.astype(F32)).astype(BF)


def mm3(a, b):
    ah, al = split2(a)
    bh, bl = split2(b)
    return mm(ah, bh) + (mm(ah, bl) + mm(al, bh))


def iotas(n, m):
    return lax.broadcasted_iota(jnp.int32, (n, m), 0), lax.broadcasted_iota(jnp.int32, (n, m), 1)


def head_ones(n):
    i, j = iotas(n, n)
    return jnp.where((i // 64) == (j // 64), 1.0, 0.0).astype(BF)


def head_sum(x, ones):
    hi, lo = split2(x)
    return mm(hi, ones) + mm(lo, ones)


def pack_map(m, b):
    i, j = iotas(128, 128)
    e = m - jnp.where(i == j, 1.0, 0.0)
    return jnp.where(j < 64, e + pltpu.roll(e, 64, 1), b + pltpu.roll(b, 64, 1)).astype(BF)


def unpack_map(p):
    i, j = iotas(128, 128)
    p = p.astype(F32)
    s = pltpu.roll(p, 64, 1)
    bd = (i // 64) == (j // 64)
    m = jnp.where(bd, jnp.where(j < 64, p, s), 0.0) + jnp.where(i == j, 1.0, 0.0)
    b = jnp.where(bd, jnp.where(j < 64, s, p), 0.0)
    return m, b


def compose(first, second):
    both = mm3(second[0], jnp.concatenate([first[0], first[1]], axis=1))
    return both[:, :128], both[:, 128:] + second[1]


def tree(level):
    while len(level) > 1:
        level = [[compose(level[z][p], level[z + 1][p]) for p in range(2)] for z in range(0, len(level), 2)]
    return level[0]


def chunk_kernel(r_ref, k_ref, v_ref, d_ref, a_ref, x_ref, q_ref, o_ref, pc_ref, mg_ref, bg_ref, pk_ref):
    step = pl.program_id(0)
    ones = head_ones(256)
    k = k_ref[...].astype(F32)
    n = k * lax.rsqrt(head_sum(k * k, ones) + 1e-6)
    rate = 1.0 / (1.0 + jnp.exp(-a_ref[...].astype(F32)))
    b = n * rate
    ld = (-0.6065306597126334) / (1.0 + jnp.exp(-d_ref[...].astype(F32))) + x_ref[...]
    i, j = iotas(ROWS, ROWS)
    tri = jnp.where(((i // CHUNK) == (j // CHUNK)) & (i >= j), 1.0, 0.0).astype(BF)
    ldh, ldl = split2(ld)
    g = mm(tri, ldh) + mm(tri, ldl)
    mids = [g[c * CHUNK + CHUNK // 2 : c * CHUNK + CHUNK // 2 + 1] for c in range(GROUP)]
    ends = [g[c * CHUNK + CHUNK - 1 : c * CHUNK + CHUNK] for c in range(GROUP)]
    rel = jnp.concatenate([g[c * CHUNK : (c + 1) * CHUNK] - mids[c] for c in range(GROUP)], axis=0)
    up = jnp.exp(rel)
    prev = jnp.exp(rel - ld)
    down = jnp.exp(-rel)
    rq = r_ref[...].astype(F32) * up
    nq = n * prev
    kk = k * down
    bb = b * down
    v = v_ref[...]

    i, j = iotas(128, 128)
    bd = (i // 64) == (j // 64)
    ti, tj = i % 64, j % 64
    strict = bd & (ti > tj)
    within = bd & (ti >= tj)
    eye = jnp.where(i == j, 1.0, 0.0)
    mask_a = jnp.concatenate([jnp.concatenate([strict, strict], axis=1), jnp.concatenate([within, within], axis=1)], axis=0)
    low = lax.broadcasted_iota(jnp.int32, (64, 128), 1) < 64
    zero = jnp.zeros((64, 128), BF)

    def spread(x):
        return jnp.concatenate([jnp.where(low, x, zero), jnp.where(low, zero, x)], axis=0)

    def fold(x):
        return jnp.where(low, x[:64], x[64:])

    units = [(c, p) for c in range(GROUP) for p in range(2)]

    def cut(x, u):
        c, p = u
        return x[c * CHUNK : (c + 1) * CHUNK, p * 128 : (p + 1) * 128]

    st = {}
    for u in units:
        nqb = spread(cut(nq, u).astype(BF))
        rqb = spread(cut(rq, u).astype(BF))
        kb = cut(kk, u).astype(BF)
        bbb = cut(bb, u).astype(BF)
        vb = cut(v, u)
        att = mm_nt(jnp.concatenate([nqb, rqb], axis=0), jnp.concatenate([kb, kb, bbb, bbb], axis=0))
        st[u] = dict(nqb=nqb, rqb=rqb, vb=vb, att=att)
    for u in units:
        t = st[u]
        att = t.pop("att")
        t["L"] = jnp.where(strict, att[:128, 128:], 0.0)
        t["arb"] = jnp.where(within, att[128:, 128:], 0.0).astype(BF)
        t["ak"] = jnp.concatenate(
            [jnp.where(strict, att[:128, :128], 0.0).astype(BF), jnp.where(within, att[128:, :128], 0.0).astype(BF)], axis=0
        )
    lev = jnp.where(bd & ((ti // 2) == (tj // 2)), 1.0, 0.0)
    for u in units:
        st[u]["X"] = eye - st[u]["L"] * lev
    s = 2
    while s < CHUNK:
        lev = ((i // (2 * s)) == (j // (2 * s))) & ((i // s) > (j // s))
        for u in units:
            x = st[u]["X"]
            xb = x.astype(BF)
            c = jnp.where(lev, st[u]["L"], 0.0).astype(BF)
            y = mm(xb, c).astype(BF)
            st[u]["X"] = x - mm(y, xb)
        s *= 2
    for u in units:
        t = st[u]
        kv = mm(t["ak"], spread(t["vb"]))
        t["av"], t["ov"] = kv[:128].astype(BF), kv[128:]
    for u in units:
        t = st[u]
        t["wu"] = mm(t["X"].astype(BF), jnp.concatenate([t["nqb"], t["av"]], axis=1))
    for u in units:
        t = st[u]
        t["f"] = mm(t["arb"], t["wu"].astype(BF))
    for u in units:
        t = st[u]
        c, p = u
        wu = t["wu"]
        tail = jnp.exp(ends[c][:, p * 128 : (p + 1) * 128] - mids[c][:, p * 128 : (p + 1) * 128])
        left = jnp.concatenate([cut(kk, u) * tail, cut(bb, u) * tail], axis=0).T.astype(BF)
        right = jnp.concatenate(
            [
                jnp.concatenate([t["vb"], zero], axis=1),
                jnp.concatenate([-fold(wu[:, 128:]), fold(wu[:, :128])], axis=1).astype(BF),
            ],
            axis=0,
        )
        t["be"] = mm(left, right)
    maps = {}
    for u in units:
        t = st[u]
        c, p = u
        f = t["f"]
        lanes = slice(p * 128, (p + 1) * 128)
        emid = jnp.exp(mids[c][:, lanes])
        q = fold(t["rqb"].astype(F32) - f[:, :128]) * emid
        rows = slice(c * CHUNK, (c + 1) * CHUNK)
        q_ref[rows, lanes] = q.astype(BF)
        o_ref[rows, lanes] = fold(t["ov"] - f[:, 128:])
        be = t["be"]
        m = jnp.where(i == j, jnp.exp(ends[c][:, lanes]), 0.0) - jnp.where(bd, be[:, 128:], 0.0) * emid
        bm = jnp.where(bd, be[:, :128], 0.0)
        maps[u] = (m, bm)
        pc_ref[step * GROUP + c, p] = pack_map(m, bm)
    level = [[maps[(c, p)] for p in range(2)] for c in range(GROUP)]
    level = tree(level)
    for p in range(2):
        mg_ref[step, p], bg_ref[step, p] = level[p]

    @pl.when(step == pl.num_programs(0) - 1)
    def _():
        level = tree([[(mg_ref[z, p], bg_ref[z, p]) for p in range(2)] for z in range(mg_ref.shape[0])])
        for p in range(2):
            pk_ref[p] = pack_map(*level[p])


def chunk_maps(r, k, v, d, a, x):
    tokens, width = r.shape
    steps = tokens // ROWS
    chunks = tokens // CHUNK
    blk = pl.BlockSpec((ROWS, width), lambda s: (s, 0))
    shapes = [
        pltpu.HBM((tokens, width), BF),
        pltpu.HBM((tokens, width), F32),
        pltpu.HBM((chunks, 2, 128, 128), BF),
        pltpu.HBM((steps, 2, 128, 128), F32),
        pltpu.HBM((steps, 2, 128, 128), F32),
        pltpu.VMEM((2, 128, 128), BF),
    ]
    return pl.pallas_call(
        chunk_kernel,
        grid=(steps,),
        in_specs=[blk] * 6,
        out_specs=[blk, blk] + [whole(s.shape) for s in shapes[2:5]] + [pl.BlockSpec(memory_space=pltpu.VMEM)],
        out_shape=shapes,
        compiler_params=pltpu.CompilerParams(dimension_semantics=("arbitrary",), vmem_limit_bytes=16 << 20),
        name="chunk_maps",
    )(*map(in_hbm, (r, k, v, d, a, x)))


def stage_kernel(count, here_ref, *refs):
    in_m_ref, in_b_ref, pk_ref, g_ref = refs[count:]
    here = here_ref[0]
    for k in range(count):
        g_ref[(here + count - k) % count] = refs[k][...]
    i, j = iotas(128, 128)
    for p in range(2):
        total = unpack_map(g_ref[0, p])
        first = here > 0
        in_m = jnp.where(first, total[0], jnp.where(i == j, 1.0, 0.0))
        in_b = jnp.where(first, total[1], 0.0)
        for k in range(1, count):
            total = compose(total, unpack_map(g_ref[k, p]))
            passed = here > k
            in_m = jnp.where(passed, total[0], in_m)
            in_b = jnp.where(passed, total[1], in_b)
        in_m_ref[p] = in_m
        in_b_ref[p] = in_b
        pk_ref[p] = pack_map(total[0], total[1])


def stage(gathered, here):
    square = pltpu.VMEM((2, 128, 128), F32)
    count = len(gathered)
    vmem = pl.BlockSpec(memory_space=pltpu.VMEM)
    return pl.pallas_call(
        lambda *refs: stage_kernel(count, *refs),
        in_specs=[pl.BlockSpec(memory_space=pltpu.SMEM)] + [vmem] * count,
        out_specs=[vmem] * 3,
        out_shape=[square, square, pltpu.VMEM((2, 128, 128), BF)],
        scratch_shapes=[pltpu.VMEM((count, 2, 128, 128), BF)],
        compiler_params=pltpu.CompilerParams(vmem_limit_bytes=4 << 20),
        name="stage",
    )(here, *map(in_vmem, gathered))


def advance(packed, state):
    i, j = iotas(128, 128)
    packed = packed.astype(F32)
    other = pltpu.roll(packed, 64, 1)
    bd = (i // 64) == (j // 64)
    e = jnp.where(bd, jnp.where(j < 64, packed, other), 0.0).astype(BF)
    b = jnp.where(bd, jnp.where(j < 64, other, packed), 0.0)
    hi, lo = split2(state)
    return state + (mm(e, hi) + mm(e, lo)) + b


def readout_kernel(count, here_ref, *refs):
    my_ref, by_ref, mx_ref, bx_ref, q_ref, o_ref, pc_ref, mg_ref, bg_ref, gate_ref, gain_ref, out_ref, ps_ref, g_ref = refs[count:]
    steps = mg_ref.shape[0]
    tokens = q_ref.shape[0]
    here = here_ref[0]
    for k in range(count):
        g_ref[(here + count - k) % count] = refs[k][...]
    cur = [jnp.zeros((128, 128), F32)] * 2
    for k in range(g_ref.shape[0] - 1):
        for p in range(2):
            m, b = unpack_map(g_ref[k, p])
            cur[p] = jnp.where(here > k, b if k == 0 else mm3(m, cur[p]) + b, cur[p])
    cur = [mm3(my_ref[p], cur[p]) + by_ref[p] for p in range(2)]
    cur = [mm3(mx_ref[p], cur[p]) + bx_ref[p] for p in range(2)]
    for g in range(steps):
        for p in range(2):
            ps_ref[g * GROUP, p] = cur[p]
            if g + 1 < steps:
                cur[p] = mm3(mg_ref[g, p], cur[p]) + bg_ref[g, p]
    for c in range(GROUP - 1):
        for g in range(steps):
            for p in range(2):
                at = g * GROUP + c
                ps_ref[at + 1, p] = advance(pc_ref[at, p], ps_ref[at, p])
    ones = head_ones(256)
    spans = [slice(b, b + ROWS) for b in range(0, tokens, ROWS)]
    outs = []
    for b in range(len(spans)):
        parts = []
        for c in range(b * GROUP, (b + 1) * GROUP):
            rows = slice(c * CHUNK, (c + 1) * CHUNK)
            parts.append(
                jnp.concatenate([mm(q_ref[rows, p * 128 : (p + 1) * 128], ps_ref[c, p].astype(BF)) for p in range(2)], axis=1)
            )
        outs.append(o_ref[spans[b]] + jnp.concatenate(parts, axis=0))
    outs = [o - head_sum(o, ones) * (1.0 / 64) for o in outs]
    sums = [head_sum(o * o, ones) * (1.0 / 64) for o in outs]
    for o, var, rows in zip(outs, sums, spans):
        y = o * lax.rsqrt(var + 0.00064) * gain_ref[...] * gate_ref[rows].astype(F32)
        out_ref[rows] = y.astype(BF)


def readout(gathered, here, maps, q, o, pc, mg, bg, gate, gain):
    tokens, width = q.shape
    count = len(gathered)
    near = (*gathered, *maps)
    far = (q, o, pc, mg, bg, gate, gain.reshape(1, width))
    vmem = pl.BlockSpec(memory_space=pltpu.VMEM)
    return pl.pallas_call(
        lambda *refs: readout_kernel(count, *refs),
        grid=(1,),
        in_specs=[pl.BlockSpec(memory_space=pltpu.SMEM)] + [vmem] * len(near) + [whole(a.shape) for a in far],
        out_specs=vmem,
        out_shape=pltpu.VMEM((tokens, width), BF),
        scratch_shapes=[pltpu.VMEM((tokens // CHUNK, 2, 128, 128), F32), pltpu.VMEM((count, 2, 128, 128), BF)],
        compiler_params=pltpu.CompilerParams(vmem_limit_bytes=16 << 20),
        name="readout",
    )(here, *map(in_vmem, near), *map(in_hbm, far))


def partial_kernel(at_ref, m_own, m_right, m_left, w_own, w_near, w_other, r_own, r_right, r_far, r_left, acc_ref):
    quarter = r_own.shape[0]
    first = at_ref[1] == 0
    for s, rows in enumerate((r_own, r_right, r_far, r_left)):
        at = pl.multiple_of((at_ref[0] + s) % 4 * quarter, quarter)
        right, left = m_right[pl.ds(at, quarter)], m_left[pl.ds(at, quarter)]
        part = mm(m_own[pl.ds(at, quarter)], w_own[...]) + mm(jnp.where(first, right, left), w_near[...])
        acc_ref[s] = rows[...].astype(F32) + (part + mm(jnp.where(first, left, right), w_other[...]))


def project_kernel(at_ref, acc_ref, m_far, w_far, w_far_other, gain_ref, normed_ref, stream_ref, edge_ref, far_s, normed_s, sems):
    _, quarter, _ = acc_ref.shape
    x, core = at_ref[0], at_ref[1]
    half = w_far.shape[0]
    far_s[pl.ds(pl.multiple_of(core * half, half), half)] = w_far[...]
    far_s[pl.ds(pl.multiple_of((1 - core) * half, half), half)] = w_far_other[...]
    writes = []
    for s in range(4):
        q = (x + s) % 4
        at = pl.multiple_of(q * quarter, quarter)
        stream = (acc_ref[s] + mm(m_far[pl.ds(at, quarter)], far_s[...])).astype(BF)
        wide = stream.astype(F32)
        scale = lax.rsqrt(jnp.mean(wide * wide, axis=-1, keepdims=True) + 1e-6)
        normed = (wide * scale * gain_ref[...]).astype(BF)
        normed_s[s] = normed
        writes.append(pltpu.make_async_copy(normed_s.at[s], normed_ref.at[pl.ds(at, quarter)], sems.at[s]))
        writes[-1].start()
        if s == 0:
            stream_ref[...] = stream

        @pl.when(q == 3)
        def _(s=s):
            edge_ref[...] = normed_s[s, quarter - HALO :]

    for c in writes:
        c.wait()


def project_partial(at, mixed, projs, rows):
    quarter, depth = rows[0].shape
    vmem = pl.BlockSpec(memory_space=pltpu.VMEM)
    near = [*mixed, *projs, *rows]
    return pl.pallas_call(
        partial_kernel,
        in_specs=[pl.BlockSpec(memory_space=pltpu.SMEM)] + [vmem] * len(near),
        out_specs=vmem,
        out_shape=pltpu.VMEM((4, quarter, depth), F32),
        compiler_params=pltpu.CompilerParams(vmem_limit_bytes=10 << 20),
        name="project_partial",
    )(at, *map(in_vmem, near))


def project(at, acc, m_far, w_far, w_far_other, gain):
    tokens, width = m_far.shape
    _, quarter, depth = acc.shape
    vmem = pl.BlockSpec(memory_space=pltpu.VMEM)
    near = [acc, m_far, w_far, w_far_other, gain.reshape(1, depth)]
    return pl.pallas_call(
        project_kernel,
        grid=(1,),
        in_specs=[pl.BlockSpec(memory_space=pltpu.SMEM)] + [vmem] * len(near),
        out_specs=[pl.BlockSpec(memory_space=pltpu.HBM), whole((quarter, depth)), vmem],
        out_shape=[pltpu.HBM((tokens, depth), BF), pltpu.HBM((quarter, depth), BF), pltpu.VMEM((HALO, depth), BF)],
        scratch_shapes=[
            pltpu.VMEM((width, depth), BF),
            pltpu.VMEM((4, quarter, depth), BF),
            pltpu.SemaphoreType.DMA((4,)),
        ],
        compiler_params=pltpu.CompilerParams(vmem_limit_bytes=16 << 20),
        name="project",
    )(at, *map(in_vmem, near))


HALO = 16
COLS = 256


def feed_kernel(offsets, load, flat, at_ref, edge_ref, taps_ref, normed_ref, weights_ref, *refs):
    if load:
        out_ref, w_ref, rows_ref, hidden_ref, pre_ref, sems = refs
    else:
        out_ref, rows_ref, hidden_ref, pre_ref, sems = refs
        w_ref = weights_ref
    quarter, depth = out_ref.shape
    width = hidden_ref.shape[1]
    steps = width // COLS
    rest = width - steps * COLS
    starts = [(f * COLS, COLS) for f in range(steps)] + ([(steps * COLS, rest)] if rest else [])
    q = (at_ref[0] + jnp.where(at_ref[1] == 0, offsets[0], offsets[1])) % 4
    before = pl.multiple_of(jnp.maximum(q * quarter - HALO, 0), HALO)
    moves = [
        (normed_ref.at[pl.ds(pl.multiple_of(q * quarter, quarter), quarter)], rows_ref.at[pl.ds(HALO, quarter)]),
        (normed_ref.at[pl.ds(before, HALO)], rows_ref.at[pl.ds(0, HALO)]),
    ]
    if load:
        for at, count in starts:
            for side in range(2):
                part = (slice(None), pl.ds(side * width + at, count))
                moves.append((weights_ref.at[part], w_ref.at[part]))
        for c in range(4):
            part = (pl.ds(c * depth // 4, depth // 4), pl.ds(2 * width, width))
            moves.append((weights_ref.at[part], w_ref.at[part]))
    copies = [pltpu.make_async_copy(a, b, sems.at[i]) for i, (a, b) in enumerate(moves)]
    for c in copies:
        c.start()
    copies[0].wait()
    copies[1].wait()
    rows_ref[:HALO] = jnp.where(q == 0, edge_ref[...], rows_ref[:HALO])

    def product(slot, at, count):
        rows = rows_ref[...]
        for side in range(2):
            cols = pl.ds(pl.multiple_of(side * width + at, 128), count)
            pre_ref[slot, side, :, :count] = mm(rows, w_ref[:, cols]).astype(BF)

    def mixing(slot, at, count):
        mixes = []
        for side in range(2):
            pre = pre_ref[slot, side, :, :count].astype(F32)
            taps = taps_ref[side, :, pl.ds(pl.multiple_of(at, 128), count)]
            mixes.append(taps[0:1] * pltpu.roll(pre, 2, 0) + taps[1:2] * pltpu.roll(pre, 1, 0) + taps[2:3] * pre)
        hid = (mixes[0] / (1.0 + jnp.exp(-mixes[0])) * mixes[1]).astype(BF)
        hidden_ref[:, pl.ds(pl.multiple_of(at, 128), count)] = hid[HALO:]

    def down(at, count):
        cols = pl.ds(pl.multiple_of(at, count), count)
        out_ref[:, cols] = mm_nt(hidden_ref[...], w_ref[cols, 2 * width :]).astype(BF)

    part = depth // 4
    if flat:
        for f, (at, count) in enumerate(starts):
            if load:
                copies[2 + 2 * f].wait()
                copies[3 + 2 * f].wait()
            product(f % 2, at, count)
            if f:
                mixing((f - 1) % 2, *starts[f - 1])
        mixing((len(starts) - 1) % 2, *starts[-1])
        for h in range(4):
            if load:
                copies[2 + 2 * len(starts) + h].wait()
            down(h * part, part)
        return
    product(0, 0, COLS)

    def turn(f, carry):
        product(f % 2, f * COLS, COLS)
        mixing((f - 1) % 2, (f - 1) * COLS, COLS)
        return carry

    lax.fori_loop(1, steps, turn, 0)
    if rest:
        product(steps % 2, *starts[-1])
    mixing((steps - 1) % 2, (steps - 1) * COLS, COLS)
    if rest:
        mixing(steps % 2, *starts[-1])

    def down_turn(h, carry):
        down(h * part, part)
        return carry

    lax.fori_loop(0, 4, down_turn, 0)


def feed(offsets, load, flat, at, normed, edge, weights, taps):
    tokens, depth = normed.shape
    quarter = tokens // 4
    width = weights.shape[1] // 3
    vmem = pl.BlockSpec(memory_space=pltpu.VMEM)
    hbm = pl.BlockSpec(memory_space=pltpu.HBM)
    out = jax.ShapeDtypeStruct((quarter, depth), BF)
    return pl.pallas_call(
        lambda *refs: feed_kernel(offsets, load, flat, *refs),
        in_specs=[pl.BlockSpec(memory_space=pltpu.SMEM), vmem, vmem, hbm, hbm if load else vmem],
        out_specs=[vmem, vmem] if load else vmem,
        scratch_shapes=[
            pltpu.VMEM((quarter + HALO, depth), BF),
            pltpu.VMEM((quarter, width), BF),
            pltpu.VMEM((2, 2, quarter + HALO, COLS), BF),
            pltpu.SemaphoreType.DMA((24 if load else 2,)),
        ],
        out_shape=[out, pltpu.VMEM(weights.shape, BF)] if load else out,
        compiler_params=pltpu.CompilerParams(vmem_limit_bytes=10 << 20),
        name="feed",
    )(at, edge, taps, in_hbm(normed), in_hbm(weights) if load else in_vmem(weights))


def shifted(x, by):
    n = lax.axis_size("tp")
    return lax.ppermute(x, "tp", [(i, (i + by) % n) for i in range(n)])


def by_core(x, first, second):
    n = lax.axis_size("tp")
    pairs = [(i, (i + first) % n) for i in range(n)] + [(n + i, n + (i + second) % n) for i in range(n)]
    return lax.ppermute(x, ("sp_2", "tp"), pairs)


def swapped(x):
    return lax.ppermute(x, "sp_2", [(0, 1), (1, 0)])


def passed_along(x, axis, by):
    count = lax.axis_size(axis)
    pairs = [(i, i + by) for i in range(count) if 0 <= i + by < count]
    return lax.ppermute(x, axis, pairs)


def everyone(x, axis):
    n = lax.axis_size(axis)
    return [x] + [lax.ppermute(x, axis, [(i, (i + by) % n) for i in range(n)]) for by in range(1, n)]


def body(
    residual_input_stream,
    receptance,
    key_matrix_all,
    value_matrix_all,
    decay_preactivation,
    learning_rate_preactivation,
    output_gate_all_heads,
    extra_log_decay,
    head_norm_gain,
    output_projection_weight,
    feedforward_norm_gain,
    gate_projection_weight,
    up_projection_weight,
    down_projection_weight,
    convolution_kernel,
):
    x = lax.axis_index("tp").astype(jnp.int32)
    core = lax.axis_index("sp_2").astype(jnp.int32)
    first = core == 0
    at = jnp.stack([x, core])
    places = [lax.axis_index(axis).astype(jnp.int32).reshape(1) for axis in SP]
    receptance, at, first, places = lax.optimization_barrier((receptance, at, first, places))
    local = jnp.concatenate([gate_projection_weight, up_projection_weight, down_projection_weight], axis=1)
    weights = lax.all_gather(local, SP, axis=0, tiled=True)
    taps = convolution_kernel.astype(F32).transpose(1, 0, 2)

    row_left, row_right = shifted(residual_input_stream, 1), shifted(residual_input_stream, -1)
    proj_near = by_core(output_projection_weight, -1, 1)

    q, o, pc, mg, bg, pk = chunk_maps(
        receptance,
        key_matrix_all,
        value_matrix_all,
        decay_preactivation,
        learning_rate_preactivation,
        extra_log_decay,
    )
    mx, bx, pk = stage(everyone(pk, "sp_2"), places[2])
    pieces = everyone(pk, "sp_1")
    my, by, pk = stage(pieces, places[1])
    half = proj_near.shape[0] // 2
    row_far = by_core(jnp.where(first, row_left, row_right), 1, -1)
    proj_far = by_core(jnp.where(first, proj_near[:half], proj_near[half:]), -1, 1)
    proj_other = swapped(proj_near)
    pieces = everyone(pk, "sp_0")
    mixed = readout(
        pieces, places[0], (my, by, mx, bx), q, o, pc, mg, bg, output_gate_all_heads, head_norm_gain
    )
    mixed_left, mixed_right = shifted(mixed, 1), shifted(mixed, -1)
    proj_far_other = swapped(proj_far)
    mixed_far = by_core(jnp.where(first, mixed_left, mixed_right), 1, -1)
    acc = project_partial(
        at,
        (mixed, mixed_right, mixed_left),
        (output_projection_weight, proj_near, proj_other),
        (residual_input_stream, row_right, row_far, row_left),
    )
    normed, stream, edge = project(at, acc, mixed_far, proj_far, proj_far_other, feedforward_norm_gain)
    edge = passed_along(edge, SP, 1)
    wide = lambda t: t.astype(F32)
    far, weights = feed((2, 2), True, True, at, normed, edge, weights, taps)
    far = by_core(far, 1, -1)
    early = by_core(feed((3, 1), False, True, at, normed, edge, weights, taps), -1, 1)
    late = feed((1, 3), False, False, at, normed, edge, weights, taps)
    late = by_core((wide(late) + wide(far)).astype(BF), 1, -1)
    own = feed((0, 0), False, False, at, normed, edge, weights, taps)
    return (wide(stream) + (wide(own) + wide(early) + wide(late))).astype(BF)


def solution(mesh):
    split = Mesh(mesh.devices.reshape(4, 4, 2, mesh.shape["tp"]), ("sp_0", "sp_1", "sp_2", "tp"))
    in_specs = (
        P(SP_TP, None),
        P(SP, "tp"),
        P(SP, "tp"),
        P(SP, "tp"),
        P(SP, "tp"),
        P(SP, "tp"),
        P(SP, "tp"),
        P(SP, "tp"),
        P("tp"),
        P("tp", None),
        P(),
        P(SP, "tp"),
        P(SP, "tp"),
        P(SP, "tp"),
        P(None, None, "tp"),
    )
    out_specs = P(SP_TP, None)

    return jax.shard_map(body, mesh=split, in_specs=in_specs, out_specs=out_specs, check_vma=False)
```

```python
import jax
import jax.numpy as jnp
from jax import lax
from jax.experimental import pallas as pl
from jax.experimental.pallas import tpu as pltpu
from jax.sharding import Mesh
from jax.sharding import PartitionSpec as P


SP = ("sp_0", "sp_1", "sp_2")
SP_TP = ("sp_0", "sp_1", "sp_2", "tp")

BF = jnp.bfloat16
F32 = jnp.float32
CHUNK = 64
GROUP = 8
ROWS = CHUNK * GROUP


def in_hbm(x):
    return pltpu.with_memory_space_constraint(x, pltpu.HBM)


def in_vmem(x):
    return pltpu.with_memory_space_constraint(x, pltpu.VMEM)


def whole(shape):
    return pl.BlockSpec(tuple(shape), lambda *_: (0,) * len(shape))


def mm(a, b):
    return lax.dot_general(a, b, (((1,), (0,)), ((), ())), preferred_element_type=F32)


def mm_nt(a, b):
    return lax.dot_general(a, b, (((1,), (1,)), ((), ())), preferred_element_type=F32)


def split2(x):
    hi = x.astype(BF)
    return hi, (x - hi.astype(F32)).astype(BF)


def mm3(a, b):
    ah, al = split2(a)
    bh, bl = split2(b)
    return mm(ah, bh) + (mm(ah, bl) + mm(al, bh))


def iotas(n, m):
    return lax.broadcasted_iota(jnp.int32, (n, m), 0), lax.broadcasted_iota(jnp.int32, (n, m), 1)


def head_ones(n):
    i, j = iotas(n, n)
    return jnp.where((i // 64) == (j // 64), 1.0, 0.0).astype(BF)


def head_sum(x, ones):
    hi, lo = split2(x)
    return mm(hi, ones) + mm(lo, ones)


def pack_map(m, b):
    i, j = iotas(128, 128)
    e = m - jnp.where(i == j, 1.0, 0.0)
    return jnp.where(j < 64, e + pltpu.roll(e, 64, 1), b + pltpu.roll(b, 64, 1)).astype(BF)


def unpack_map(p):
    i, j = iotas(128, 128)
    p = p.astype(F32)
    s = pltpu.roll(p, 64, 1)
    bd = (i // 64) == (j // 64)
    m = jnp.where(bd, jnp.where(j < 64, p, s), 0.0) + jnp.where(i == j, 1.0, 0.0)
    b = jnp.where(bd, jnp.where(j < 64, s, p), 0.0)
    return m, b


def compose(first, second):
    both = mm3(second[0], jnp.concatenate([first[0], first[1]], axis=1))
    return both[:, :128], both[:, 128:] + second[1]


def tree(level):
    while len(level) > 1:
        level = [[compose(level[z][p], level[z + 1][p]) for p in range(2)] for z in range(0, len(level), 2)]
    return level[0]


def chunk_kernel(r_ref, k_ref, v_ref, d_ref, a_ref, x_ref, q_ref, o_ref, pc_ref, mg_ref, bg_ref, pk_ref):
    step = pl.program_id(0)
    ones = head_ones(256)
    k = k_ref[...].astype(F32)
    n = k * lax.rsqrt(head_sum(k * k, ones) + 1e-6)
    rate = 1.0 / (1.0 + jnp.exp(-a_ref[...].astype(F32)))
    b = n * rate
    ld = (-0.6065306597126334) / (1.0 + jnp.exp(-d_ref[...].astype(F32))) + x_ref[...]
    i, j = iotas(ROWS, ROWS)
    tri = jnp.where(((i // CHUNK) == (j // CHUNK)) & (i >= j), 1.0, 0.0).astype(BF)
    ldh, ldl = split2(ld)
    g = mm(tri, ldh) + mm(tri, ldl)
    mids = [g[c * CHUNK + CHUNK // 2 : c * CHUNK + CHUNK // 2 + 1] for c in range(GROUP)]
    ends = [g[c * CHUNK + CHUNK - 1 : c * CHUNK + CHUNK] for c in range(GROUP)]
    rel = jnp.concatenate([g[c * CHUNK : (c + 1) * CHUNK] - mids[c] for c in range(GROUP)], axis=0)
    up = jnp.exp(rel)
    prev = jnp.exp(rel - ld)
    down = jnp.exp(-rel)
    rq = r_ref[...].astype(F32) * up
    nq = n * prev
    kk = k * down
    bb = b * down
    v = v_ref[...]

    i, j = iotas(128, 128)
    bd = (i // 64) == (j // 64)
    ti, tj = i % 64, j % 64
    strict = bd & (ti > tj)
    within = bd & (ti >= tj)
    eye = jnp.where(i == j, 1.0, 0.0)
    mask_a = jnp.concatenate([jnp.concatenate([strict, strict], axis=1), jnp.concatenate([within, within], axis=1)], axis=0)
    low = lax.broadcasted_iota(jnp.int32, (64, 128), 1) < 64
    zero = jnp.zeros((64, 128), BF)

    def spread(x):
        return jnp.concatenate([jnp.where(low, x, zero), jnp.where(low, zero, x)], axis=0)

    def fold(x):
        return jnp.where(low, x[:64], x[64:])

    units = [(c, p) for c in range(GROUP) for p in range(2)]

    def cut(x, u):
        c, p = u
        return x[c * CHUNK : (c + 1) * CHUNK, p * 128 : (p + 1) * 128]

    st = {}
    for u in units:
        nqb = spread(cut(nq, u).astype(BF))
        rqb = spread(cut(rq, u).astype(BF))
        kb = cut(kk, u).astype(BF)
        bbb = cut(bb, u).astype(BF)
        vb = cut(v, u)
        att = mm_nt(jnp.concatenate([nqb, rqb], axis=0), jnp.concatenate([kb, kb, bbb, bbb], axis=0))
        st[u] = dict(nqb=nqb, rqb=rqb, vb=vb, att=att)
    for u in units:
        t = st[u]
        att = t.pop("att")
        t["L"] = jnp.where(strict, att[:128, 128:], 0.0)
        t["arb"] = jnp.where(within, att[128:, 128:], 0.0).astype(BF)
        t["ak"] = jnp.concatenate(
            [jnp.where(strict, att[:128, :128], 0.0).astype(BF), jnp.where(within, att[128:, :128], 0.0).astype(BF)], axis=0
        )
    lev = jnp.where(bd & ((ti // 2) == (tj // 2)), 1.0, 0.0)
    for u in units:
        st[u]["X"] = eye - st[u]["L"] * lev
    s = 2
    while s < CHUNK:
        lev = ((i // (2 * s)) == (j // (2 * s))) & ((i // s) > (j // s))
        for u in units:
            x = st[u]["X"]
            xb = x.astype(BF)
            c = jnp.where(lev, st[u]["L"], 0.0).astype(BF)
            y = mm(xb, c).astype(BF)
            st[u]["X"] = x - mm(y, xb)
        s *= 2
    for u in units:
        t = st[u]
        kv = mm(t["ak"], spread(t["vb"]))
        t["av"], t["ov"] = kv[:128].astype(BF), kv[128:]
    for u in units:
        t = st[u]
        t["wu"] = mm(t["X"].astype(BF), jnp.concatenate([t["nqb"], t["av"]], axis=1))
    for u in units:
        t = st[u]
        t["f"] = mm(t["arb"], t["wu"].astype(BF))
    for u in units:
        t = st[u]
        c, p = u
        wu = t["wu"]
        tail = jnp.exp(ends[c][:, p * 128 : (p + 1) * 128] - mids[c][:, p * 128 : (p + 1) * 128])
        left = jnp.concatenate([cut(kk, u) * tail, cut(bb, u) * tail], axis=0).T.astype(BF)
        right = jnp.concatenate(
            [
                jnp.concatenate([t["vb"], zero], axis=1),
                jnp.concatenate([-fold(wu[:, 128:]), fold(wu[:, :128])], axis=1).astype(BF),
            ],
            axis=0,
        )
        t["be"] = mm(left, right)
    maps = {}
    for u in units:
        t = st[u]
        c, p = u
        f = t["f"]
        lanes = slice(p * 128, (p + 1) * 128)
        emid = jnp.exp(mids[c][:, lanes])
        q = fold(t["rqb"].astype(F32) - f[:, :128]) * emid
        rows = slice(c * CHUNK, (c + 1) * CHUNK)
        q_ref[rows, lanes] = q.astype(BF)
        o_ref[rows, lanes] = fold(t["ov"] - f[:, 128:])
        be = t["be"]
        m = jnp.where(i == j, jnp.exp(ends[c][:, lanes]), 0.0) - jnp.where(bd, be[:, 128:], 0.0) * emid
        bm = jnp.where(bd, be[:, :128], 0.0)
        maps[u] = (m, bm)
        pc_ref[step * GROUP + c, p] = pack_map(m, bm)
    level = [[maps[(c, p)] for p in range(2)] for c in range(GROUP)]
    level = tree(level)
    for p in range(2):
        mg_ref[step, p], bg_ref[step, p] = level[p]

    @pl.when(step == pl.num_programs(0) - 1)
    def _():
        level = tree([[(mg_ref[z, p], bg_ref[z, p]) for p in range(2)] for z in range(mg_ref.shape[0])])
        for p in range(2):
            pk_ref[p] = pack_map(*level[p])


def chunk_maps(r, k, v, d, a, x):
    tokens, width = r.shape
    steps = tokens // ROWS
    chunks = tokens // CHUNK
    blk = pl.BlockSpec((ROWS, width), lambda s: (s, 0))
    shapes = [
        pltpu.HBM((tokens, width), BF),
        pltpu.HBM((tokens, width), F32),
        pltpu.HBM((chunks, 2, 128, 128), BF),
        pltpu.HBM((steps, 2, 128, 128), F32),
        pltpu.HBM((steps, 2, 128, 128), F32),
        pltpu.VMEM((2, 128, 128), BF),
    ]
    return pl.pallas_call(
        chunk_kernel,
        grid=(steps,),
        in_specs=[blk] * 6,
        out_specs=[blk, blk] + [whole(s.shape) for s in shapes[2:5]] + [pl.BlockSpec(memory_space=pltpu.VMEM)],
        out_shape=shapes,
        compiler_params=pltpu.CompilerParams(dimension_semantics=("arbitrary",), vmem_limit_bytes=16 << 20),
        name="chunk_maps",
    )(*map(in_hbm, (r, k, v, d, a, x)))


def stage_kernel(count, here_ref, *refs):
    in_m_ref, in_b_ref, pk_ref, g_ref = refs[count:]
    here = here_ref[0]
    for k in range(count):
        g_ref[(here + count - k) % count] = refs[k][...]
    i, j = iotas(128, 128)
    for p in range(2):
        total = unpack_map(g_ref[0, p])
        first = here > 0
        in_m = jnp.where(first, total[0], jnp.where(i == j, 1.0, 0.0))
        in_b = jnp.where(first, total[1], 0.0)
        for k in range(1, count):
            total = compose(total, unpack_map(g_ref[k, p]))
            passed = here > k
            in_m = jnp.where(passed, total[0], in_m)
            in_b = jnp.where(passed, total[1], in_b)
        in_m_ref[p] = in_m
        in_b_ref[p] = in_b
        pk_ref[p] = pack_map(total[0], total[1])


def stage(gathered, here):
    square = pltpu.VMEM((2, 128, 128), F32)
    count = len(gathered)
    vmem = pl.BlockSpec(memory_space=pltpu.VMEM)
    return pl.pallas_call(
        lambda *refs: stage_kernel(count, *refs),
        in_specs=[pl.BlockSpec(memory_space=pltpu.SMEM)] + [vmem] * count,
        out_specs=[vmem] * 3,
        out_shape=[square, square, pltpu.VMEM((2, 128, 128), BF)],
        scratch_shapes=[pltpu.VMEM((count, 2, 128, 128), BF)],
        compiler_params=pltpu.CompilerParams(vmem_limit_bytes=4 << 20),
        name="stage",
    )(here, *map(in_vmem, gathered))


def advance(packed, state):
    i, j = iotas(128, 128)
    packed = packed.astype(F32)
    other = pltpu.roll(packed, 64, 1)
    bd = (i // 64) == (j // 64)
    e = jnp.where(bd, jnp.where(j < 64, packed, other), 0.0).astype(BF)
    b = jnp.where(bd, jnp.where(j < 64, other, packed), 0.0)
    hi, lo = split2(state)
    return state + (mm(e, hi) + mm(e, lo)) + b


def readout_kernel(count, here_ref, *refs):
    my_ref, by_ref, mx_ref, bx_ref, q_ref, o_ref, pc_ref, mg_ref, bg_ref, gate_ref, gain_ref, out_ref, ps_ref, g_ref = refs[count:]
    steps = mg_ref.shape[0]
    tokens = q_ref.shape[0]
    here = here_ref[0]
    for k in range(count):
        g_ref[(here + count - k) % count] = refs[k][...]
    cur = [jnp.zeros((128, 128), F32)] * 2
    for k in range(g_ref.shape[0] - 1):
        for p in range(2):
            m, b = unpack_map(g_ref[k, p])
            cur[p] = jnp.where(here > k, b if k == 0 else mm3(m, cur[p]) + b, cur[p])
    cur = [mm3(my_ref[p], cur[p]) + by_ref[p] for p in range(2)]
    cur = [mm3(mx_ref[p], cur[p]) + bx_ref[p] for p in range(2)]
    for g in range(steps):
        for p in range(2):
            ps_ref[g * GROUP, p] = cur[p]
            if g + 1 < steps:
                cur[p] = mm3(mg_ref[g, p], cur[p]) + bg_ref[g, p]
    for c in range(GROUP - 1):
        for g in range(steps):
            for p in range(2):
                at = g * GROUP + c
                ps_ref[at + 1, p] = advance(pc_ref[at, p], ps_ref[at, p])
    ones = head_ones(256)
    spans = [slice(b, b + ROWS) for b in range(0, tokens, ROWS)]
    outs = []
    for b in range(len(spans)):
        parts = []
        for c in range(b * GROUP, (b + 1) * GROUP):
            rows = slice(c * CHUNK, (c + 1) * CHUNK)
            parts.append(
                jnp.concatenate([mm(q_ref[rows, p * 128 : (p + 1) * 128], ps_ref[c, p].astype(BF)) for p in range(2)], axis=1)
            )
        outs.append(o_ref[spans[b]] + jnp.concatenate(parts, axis=0))
    outs = [o - head_sum(o, ones) * (1.0 / 64) for o in outs]
    sums = [head_sum(o * o, ones) * (1.0 / 64) for o in outs]
    for o, var, rows in zip(outs, sums, spans):
        y = o * lax.rsqrt(var + 0.00064) * gain_ref[...] * gate_ref[rows].astype(F32)
        out_ref[rows] = y.astype(BF)


def readout(gathered, here, maps, q, o, pc, mg, bg, gate, gain):
    tokens, width = q.shape
    count = len(gathered)
    near = (*gathered, *maps)
    far = (q, o, pc, mg, bg, gate, gain.reshape(1, width))
    vmem = pl.BlockSpec(memory_space=pltpu.VMEM)
    return pl.pallas_call(
        lambda *refs: readout_kernel(count, *refs),
        grid=(1,),
        in_specs=[pl.BlockSpec(memory_space=pltpu.SMEM)] + [vmem] * len(near) + [whole(a.shape) for a in far],
        out_specs=vmem,
        out_shape=pltpu.VMEM((tokens, width), BF),
        scratch_shapes=[pltpu.VMEM((tokens // CHUNK, 2, 128, 128), F32), pltpu.VMEM((count, 2, 128, 128), BF)],
        compiler_params=pltpu.CompilerParams(vmem_limit_bytes=16 << 20),
        name="readout",
    )(here, *map(in_vmem, near), *map(in_hbm, far))


def partial_kernel(at_ref, m_own, m_right, m_left, w_own, w_near, w_other, r_own, r_right, r_far, r_left, acc_ref):
    quarter = r_own.shape[0]
    first = at_ref[1] == 0
    for s, rows in enumerate((r_own, r_right, r_far, r_left)):
        at = pl.multiple_of((at_ref[0] + s) % 4 * quarter, quarter)
        right, left = m_right[pl.ds(at, quarter)], m_left[pl.ds(at, quarter)]
        part = mm(m_own[pl.ds(at, quarter)], w_own[...]) + mm(jnp.where(first, right, left), w_near[...])
        acc_ref[s] = rows[...].astype(F32) + (part + mm(jnp.where(first, left, right), w_other[...]))


def project_kernel(at_ref, acc_ref, m_far, w_far, w_far_other, gain_ref, normed_ref, stream_ref, edge_ref, far_s, normed_s, sems):
    _, quarter, _ = acc_ref.shape
    x, core = at_ref[0], at_ref[1]
    half = w_far.shape[0]
    far_s[pl.ds(pl.multiple_of(core * half, half), half)] = w_far[...]
    far_s[pl.ds(pl.multiple_of((1 - core) * half, half), half)] = w_far_other[...]

    def write(s):
        at = pl.multiple_of((x + s) % 4 * quarter, quarter)
        return pltpu.make_async_copy(normed_s.at[s], normed_ref.at[pl.ds(at, quarter)], sems.at[s])

    def turn(s, carry):
        q = (x + s) % 4
        at = pl.multiple_of(q * quarter, quarter)
        stream = (acc_ref[s] + mm(m_far[pl.ds(at, quarter)], far_s[...])).astype(BF)
        wide = stream.astype(F32)
        scale = lax.rsqrt(jnp.mean(wide * wide, axis=-1, keepdims=True) + 1e-6)
        normed_s[s] = (wide * scale * gain_ref[...]).astype(BF)
        write(s).start()

        @pl.when(s == 0)
        def _():
            stream_ref[...] = stream

        @pl.when(q == 3)
        def _():
            edge_ref[...] = normed_s[s, quarter - HALO :]

        return carry

    lax.fori_loop(0, 4, turn, 0)
    for s in range(4):
        write(s).wait()


def project_partial(at, mixed, projs, rows):
    quarter, depth = rows[0].shape
    vmem = pl.BlockSpec(memory_space=pltpu.VMEM)
    near = [*mixed, *projs, *rows]
    return pl.pallas_call(
        partial_kernel,
        in_specs=[pl.BlockSpec(memory_space=pltpu.SMEM)] + [vmem] * len(near),
        out_specs=vmem,
        out_shape=pltpu.VMEM((4, quarter, depth), F32),
        compiler_params=pltpu.CompilerParams(vmem_limit_bytes=10 << 20),
        name="project_partial",
    )(at, *map(in_vmem, near))


def project(at, acc, m_far, w_far, w_far_other, gain):
    tokens, width = m_far.shape
    _, quarter, depth = acc.shape
    vmem = pl.BlockSpec(memory_space=pltpu.VMEM)
    near = [acc, m_far, w_far, w_far_other, gain.reshape(1, depth)]
    return pl.pallas_call(
        project_kernel,
        grid=(1,),
        in_specs=[pl.BlockSpec(memory_space=pltpu.SMEM)] + [vmem] * len(near),
        out_specs=[pl.BlockSpec(memory_space=pltpu.HBM), whole((quarter, depth)), vmem],
        out_shape=[pltpu.HBM((tokens, depth), BF), pltpu.HBM((quarter, depth), BF), pltpu.VMEM((HALO, depth), BF)],
        scratch_shapes=[
            pltpu.VMEM((width, depth), BF),
            pltpu.VMEM((4, quarter, depth), BF),
            pltpu.SemaphoreType.DMA((4,)),
        ],
        compiler_params=pltpu.CompilerParams(vmem_limit_bytes=16 << 20),
        name="project",
    )(at, *map(in_vmem, near))


HALO = 16
COLS = 256


def feed_kernel(offsets, load, flat, COLS, at_ref, edge_ref, taps_ref, normed_ref, weights_ref, *refs):
    if load:
        out_ref, w_ref, rows_ref, hidden_ref, pre_ref, sems = refs
    else:
        out_ref, rows_ref, hidden_ref, pre_ref, sems = refs
        w_ref = weights_ref
    quarter, depth = out_ref.shape
    width = hidden_ref.shape[1]
    steps = width // COLS
    rest = width - steps * COLS
    starts = [(f * COLS, COLS) for f in range(steps)] + ([(steps * COLS, rest)] if rest else [])
    q = (at_ref[0] + jnp.where(at_ref[1] == 0, offsets[0], offsets[1])) % 4
    before = pl.multiple_of(jnp.maximum(q * quarter - HALO, 0), HALO)
    moves = [
        (normed_ref.at[pl.ds(pl.multiple_of(q * quarter, quarter), quarter)], rows_ref.at[pl.ds(HALO, quarter)]),
        (normed_ref.at[pl.ds(before, HALO)], rows_ref.at[pl.ds(0, HALO)]),
    ]
    if load:
        for at, count in starts:
            for side in range(2):
                part = (slice(None), pl.ds(side * width + at, count))
                moves.append((weights_ref.at[part], w_ref.at[part]))
        for c in range(4):
            part = (pl.ds(c * depth // 4, depth // 4), pl.ds(2 * width, width))
            moves.append((weights_ref.at[part], w_ref.at[part]))
    copies = [pltpu.make_async_copy(a, b, sems.at[i]) for i, (a, b) in enumerate(moves)]
    for c in copies:
        c.start()
    copies[0].wait()
    copies[1].wait()
    rows_ref[:HALO] = jnp.where(q == 0, edge_ref[...], rows_ref[:HALO])

    def product(slot, at, count):
        rows = rows_ref[...]
        for side in range(2):
            cols = pl.ds(pl.multiple_of(side * width + at, 128), count)
            pre_ref[slot, side, :, :count] = mm(rows, w_ref[:, cols]).astype(BF)

    def mixing(slot, at, count):
        mixes = []
        for side in range(2):
            pre = pre_ref[slot, side, :, :count].astype(F32)
            taps = taps_ref[side, :, pl.ds(pl.multiple_of(at, 128), count)]
            mixes.append(taps[0:1] * pltpu.roll(pre, 2, 0) + taps[1:2] * pltpu.roll(pre, 1, 0) + taps[2:3] * pre)
        hid = (mixes[0] / (1.0 + jnp.exp(-mixes[0])) * mixes[1]).astype(BF)
        hidden_ref[:, pl.ds(pl.multiple_of(at, 128), count)] = hid[HALO:]

    def down(at, count):
        cols = pl.ds(pl.multiple_of(at, count), count)
        out_ref[:, cols] = mm_nt(hidden_ref[...], w_ref[cols, 2 * width :]).astype(BF)

    part = depth // 4
    if flat:
        for f, (at, count) in enumerate(starts):
            if load:
                copies[2 + 2 * f].wait()
                copies[3 + 2 * f].wait()
            product(f % 2, at, count)
            if f:
                mixing((f - 1) % 2, *starts[f - 1])
        mixing((len(starts) - 1) % 2, *starts[-1])
        for h in range(4):
            if load:
                copies[2 + 2 * len(starts) + h].wait()
            down(h * part, part)
        return
    product(0, 0, COLS)

    def turn(f, carry):
        product(f % 2, f * COLS, COLS)
        mixing((f - 1) % 2, (f - 1) * COLS, COLS)
        return carry

    lax.fori_loop(1, steps, turn, 0)
    if rest:
        product(steps % 2, *starts[-1])
    mixing((steps - 1) % 2, (steps - 1) * COLS, COLS)
    if rest:
        mixing(steps % 2, *starts[-1])

    def down_turn(h, carry):
        down(h * part, part)
        return carry

    part = min(part, 2 * COLS)
    lax.fori_loop(0, depth // part, down_turn, 0)


def feed(offsets, load, flat, at, normed, edge, weights, taps, cols=COLS):
    tokens, depth = normed.shape
    quarter = tokens // 4
    width = weights.shape[1] // 3
    vmem = pl.BlockSpec(memory_space=pltpu.VMEM)
    hbm = pl.BlockSpec(memory_space=pltpu.HBM)
    out = jax.ShapeDtypeStruct((quarter, depth), BF)
    return pl.pallas_call(
        lambda *refs: feed_kernel(offsets, load, flat, cols, *refs),
        in_specs=[pl.BlockSpec(memory_space=pltpu.SMEM), vmem, vmem, hbm, hbm if load else vmem],
        out_specs=[vmem, vmem] if load else vmem,
        scratch_shapes=[
            pltpu.VMEM((quarter + HALO, depth), BF),
            pltpu.VMEM((quarter, width), BF),
            pltpu.VMEM((2, 2, quarter + HALO, cols), BF),
            pltpu.SemaphoreType.DMA((24 if load else 2,)),
        ],
        out_shape=[out, pltpu.VMEM(weights.shape, BF)] if load else out,
        compiler_params=pltpu.CompilerParams(vmem_limit_bytes=10 << 20),
        name="feed",
    )(at, edge, taps, in_hbm(normed), in_hbm(weights) if load else in_vmem(weights))


def shifted(x, by):
    n = lax.axis_size("tp")
    return lax.ppermute(x, "tp", [(i, (i + by) % n) for i in range(n)])


def by_core(x, first, second):
    n = lax.axis_size("tp")
    pairs = [(i, (i + first) % n) for i in range(n)] + [(n + i, n + (i + second) % n) for i in range(n)]
    return lax.ppermute(x, ("sp_2", "tp"), pairs)


def swapped(x):
    return lax.ppermute(x, "sp_2", [(0, 1), (1, 0)])


def passed_along(x, axis, by):
    count = lax.axis_size(axis)
    pairs = [(i, i + by) for i in range(count) if 0 <= i + by < count]
    return lax.ppermute(x, axis, pairs)


def everyone(x, axis):
    n = lax.axis_size(axis)
    return [x] + [lax.ppermute(x, axis, [(i, (i + by) % n) for i in range(n)]) for by in range(1, n)]


def body(
    residual_input_stream,
    receptance,
    key_matrix_all,
    value_matrix_all,
    decay_preactivation,
    learning_rate_preactivation,
    output_gate_all_heads,
    extra_log_decay,
    head_norm_gain,
    output_projection_weight,
    feedforward_norm_gain,
    gate_projection_weight,
    up_projection_weight,
    down_projection_weight,
    convolution_kernel,
):
    x = lax.axis_index("tp").astype(jnp.int32)
    core = lax.axis_index("sp_2").astype(jnp.int32)
    first = core == 0
    at = jnp.stack([x, core])
    places = [lax.axis_index(axis).astype(jnp.int32).reshape(1) for axis in SP]
    receptance, at, first, places = lax.optimization_barrier((receptance, at, first, places))
    local = jnp.concatenate([gate_projection_weight, up_projection_weight, down_projection_weight], axis=1)
    weights = lax.all_gather(local, SP, axis=0, tiled=True)
    taps = convolution_kernel.astype(F32).transpose(1, 0, 2)

    row_left, row_right = shifted(residual_input_stream, 1), shifted(residual_input_stream, -1)
    proj_near = by_core(output_projection_weight, -1, 1)

    q, o, pc, mg, bg, pk = chunk_maps(
        receptance,
        key_matrix_all,
        value_matrix_all,
        decay_preactivation,
        learning_rate_preactivation,
        extra_log_decay,
    )
    mx, bx, pk = stage(everyone(pk, "sp_2"), places[2])
    pieces = everyone(pk, "sp_1")
    my, by, pk = stage(pieces, places[1])
    half = proj_near.shape[0] // 2
    row_far = by_core(jnp.where(first, row_left, row_right), 1, -1)
    proj_far = by_core(jnp.where(first, proj_near[:half], proj_near[half:]), -1, 1)
    proj_other = swapped(proj_near)
    pieces = everyone(pk, "sp_0")
    mixed = readout(
        pieces, places[0], (my, by, mx, bx), q, o, pc, mg, bg, output_gate_all_heads, head_norm_gain
    )
    mixed_left, mixed_right = shifted(mixed, 1), shifted(mixed, -1)
    proj_far_other = swapped(proj_far)
    mixed_far = by_core(jnp.where(first, mixed_left, mixed_right), 1, -1)
    acc = project_partial(
        at,
        (mixed, mixed_right, mixed_left),
        (output_projection_weight, proj_near, proj_other),
        (residual_input_stream, row_right, row_far, row_left),
    )
    normed, stream, edge = project(at, acc, mixed_far, proj_far, proj_far_other, feedforward_norm_gain)
    edge = passed_along(edge, SP, 1)
    wide = lambda t: t.astype(F32)
    far, weights = feed((2, 2), True, True, at, normed, edge, weights, taps)
    far = by_core(far, 1, -1)
    early = by_core(feed((3, 1), False, True, at, normed, edge, weights, taps), -1, 1)
    late = feed((1, 3), False, False, at, normed, edge, weights, taps)
    late = by_core((wide(late) + wide(far)).astype(BF), 1, -1)
    own = feed((0, 0), False, False, at, normed, edge, weights, taps, cols=128)
    return (wide(stream) + (wide(own) + wide(early) + wide(late))).astype(BF)


def solution(mesh):
    split = Mesh(mesh.devices.reshape(4, 4, 2, mesh.shape["tp"]), ("sp_0", "sp_1", "sp_2", "tp"))
    in_specs = (
        P(SP_TP, None),
        P(SP, "tp"),
        P(SP, "tp"),
        P(SP, "tp"),
        P(SP, "tp"),
        P(SP, "tp"),
        P(SP, "tp"),
        P(SP, "tp"),
        P("tp"),
        P("tp", None),
        P(),
        P(SP, "tp"),
        P(SP, "tp"),
        P(SP, "tp"),
        P(None, None, "tp"),
    )
    out_specs = P(SP_TP, None)

    return jax.shard_map(body, mesh=split, in_specs=in_specs, out_specs=out_specs, check_vma=False)
```
